256 devices in a mesh: dp: 4 (over y), kv: 32 (over z, x), tp: 2 (over core).
Axes of the slice: x: 4, y: 4, z: 8, core: 2. Of those that a mesh axis runs over, the one named last changes fastest.
Arguments:
- tokens: bfloat16 [32768, 2048], P(('dp', 'kv'), 'tp'), parts along dimension 0, may hold values from -6 to 6
- query_weight: bfloat16 [2048, 1024], P(None, 'tp'), may hold values from -2 to 2
- key_weight: bfloat16 [2048, 1024], P(None, 'tp'), may hold values from -2 to 2
- value_weight: bfloat16 [2048, 1024], P(None, 'tp'), may hold values from -0.125 to 0.125
- out_weight: bfloat16 [1024, 2048], P(None, 'tp'), may hold values from -0.75 to 0.75
- chosen: int32 [1024, 16], P(('dp', 'kv')), parts along dimension 0, may hold values from -1 to 255, as said below
Outputs:
- mixed: bfloat16 [32768, 2048], P(('dp', 'kv'), 'tp'), parts along dimension 0
The draws below stay inside these ranges and needn't reach their ends.
There are 4 independent parts, one for each index of `dp`. The reference program is written for one: setup_inputs(seed, part) draws one part's arguments, and reference() takes and returns one part's arrays. A program takes and returns all parts, laid end to end along the dimension named above; an argument that names none is the same for every part. Nothing has to cross between parts.
Inputs may be any that keep to these rules, and one draw needn't show every extreme that they name: Each row of chosen lists distinct key blocks no later than its own query block, followed or mixed with -1 for empty slots; the own block is always listed, and block 0 too. For the 8 query blocks of one index of kv (aligned runs of rows), the distinct listed key blocks that lie among the 8 blocks of any one other index number at most 3, and exactly 3 for the index just before.
All inputs are finite; a program needn't handle non-finite values.
Results may differ from the reference program's by a relative error of at most 0.0084.
Values may be sent and summed in bfloat16 or wider, within the bound.
A program may use at most 128 MiB of HBM per device.

```python
import jax
import jax.numpy as jnp
from jax import lax

D = 2048
HEADS = 16
HEAD_DIM = 64
BLOCK = 32
TOPK = 16
CAP = 3
HW = 1024
BLK_DEV = 8
LEN = 8192
NBLK = 256


def paired_weights(key):
    first_key, second_key = jax.random.split(jax.random.fold_in(key, 5), 2)
    fan_scale = D ** (-0.5)
    base_draw = jax.random.normal(first_key, (D, HW), jnp.float32)
    other_draw = jax.random.normal(second_key, (D, HW), jnp.float32)
    query_part = base_draw
    key_part = other_draw
    return (jnp.clip(query_part * fan_scale, -2.0, 2.0), jnp.clip(key_part * fan_scale, -2.0, 2.0))


def draw_query_weight(key, part):
    return paired_weights(key)[0].astype(jnp.bfloat16)


def draw_key_weight(key, part):
    return paired_weights(key)[1].astype(jnp.bfloat16)


def draw_chosen(key, part):
    devices = NBLK // BLK_DEV
    key_popular, key_pick, key_score = jax.random.split(jax.random.fold_in(key, 11), 3)
    block_ids = jnp.arange(NBLK, dtype=jnp.int32)
    owner = block_ids // BLK_DEV
    local_index = block_ids % BLK_DEV
    popular = (jax.random.randint(key_popular, (NBLK,), 0, 8) == 0).astype(jnp.int32)
    asker = jnp.arange(devices, dtype=jnp.int32)[:, None]
    pick_score = jax.random.randint(key_pick, (devices, NBLK), 0, 4096) + popular[None, :] * 8192
    forced = (owner[None, :] == asker - 1) & (local_index[None, :] == BLK_DEV - 1) | (block_ids[None, :] == 0)
    pick_score = jnp.where(forced, 16384, pick_score) * BLK_DEV + (BLK_DEV - 1 - local_index)[None, :]
    pick_grid = pick_score.reshape(devices, devices, BLK_DEV)
    rank_in = jnp.sum((pick_grid[..., None, :] > pick_grid[..., :, None]).astype(jnp.int32), axis=-1)
    holder_ids = jnp.arange(devices, dtype=jnp.int32)
    allowed = (rank_in < CAP) & (holder_ids[None, :, None] < asker[:, :, None])
    allowed = allowed.reshape(devices, NBLK)
    query_block = block_ids[:, None]
    key_block = block_ids[None, :]
    query_owner = query_block // BLK_DEV
    local_ok = (key_block // BLK_DEV == query_owner) & (key_block <= query_block)
    remote_ok = allowed[query_owner[:, 0]]
    valid = local_ok | remote_ok
    mandatory = (key_block == query_block) | remote_ok & (key_block // BLK_DEV == query_owner - 1)
    mandatory = mandatory | (key_block == 0) & valid
    noise = jax.random.randint(key_score, (NBLK, NBLK), 0, 4096) + popular[None, :] * 4096
    score_int = jnp.where(mandatory, 16384, noise)
    score_int = jnp.where(valid, score_int * NBLK + key_block, -1)
    top_values, top_index = lax.top_k(score_int, TOPK)
    return jnp.where(top_values >= 0, top_index, -1).astype(jnp.int32)


def levels(own_key, shape, cuts, low, top_value):
    loudness, own = 1.0, jax.random.fold_in(own_key, 6)
    for position, parts in cuts:
        steps = jnp.exp(jax.random.uniform(jax.random.fold_in(own, position), (parts,), jnp.float32, low / len(cuts), top_value / len(cuts)))
        loudness = loudness * jnp.repeat(steps, shape[position] // parts).reshape([-1 if axis == position else 1 for axis in range(len(shape))])
    return loudness


def centred(rng, shape, spread, reach, cuts=(), kind=jnp.bfloat16):
    result = spread * jax.random.normal(rng, shape, jnp.float32)
    if cuts:
        result = result * levels(rng, shape, cuts, -0.22, 0.18)
    return jnp.clip(result, -reach, reach).astype(kind)


def setup_inputs(seed: int = 0, part: int = 0) -> dict:
    arg_keys = jax.random.split(jax.random.key(seed), 7)
    part_keys = jax.random.split(jax.random.fold_in(arg_keys[6], part), 7)
    return {
        "tokens": centred(part_keys[0], (LEN, D), 1.0, 6.0, ((0, 32), (1, 2))),
        "query_weight": draw_query_weight(jax.random.fold_in(arg_keys[6], 71), part),
        "key_weight": draw_key_weight(jax.random.fold_in(arg_keys[6], 71), part),
        "value_weight": centred(arg_keys[3], (D, HW), D ** -0.5, 0.125, ((1, 2),)),
        "out_weight": centred(arg_keys[4], (HW, D), (HW // 16) ** -0.5, 0.75, ((1, 2),)),
        "chosen": draw_chosen(jax.random.fold_in(jax.random.fold_in(arg_keys[6], part), 71), part),
    }


rotary_base = 500000.0
masked_score = -1e30


def rotate(heads_in, positions):
    half_dim = heads_in.shape[-1] // 2
    inverse = 1.0 / (rotary_base ** (jnp.arange(half_dim, dtype=jnp.float32) / half_dim))
    angles = positions.astype(jnp.float32)[:, None] * inverse[None, :]
    cosine = jnp.cos(angles)[:, None, :]
    sine_part = jnp.sin(angles)[:, None, :]
    first_half = heads_in[..., :half_dim]
    second_half = heads_in[..., half_dim:]
    return jnp.concatenate([first_half * cosine - second_half * sine_part,
                            first_half * sine_part + second_half * cosine], axis=-1)


def reference(tokens, query_weight, key_weight, value_weight, out_weight, chosen):
    length = tokens.shape[0]
    positions = jnp.arange(length, dtype=jnp.int32)
    heads_shape = (length, HEADS, HEAD_DIM)
    query_proj = rotate(jnp.dot(tokens, query_weight, preferred_element_type=jnp.float32).reshape(heads_shape),
                        positions).astype(jnp.bfloat16)
    key_proj = rotate(jnp.dot(tokens, key_weight, preferred_element_type=jnp.float32).reshape(heads_shape),
                      positions).astype(jnp.bfloat16)
    value_proj = jnp.dot(tokens, value_weight, preferred_element_type=jnp.float32).astype(jnp.bfloat16).reshape(heads_shape)
    blocks = length // BLOCK
    key_blocks = key_proj.reshape(blocks, BLOCK, HEADS, HEAD_DIM)
    value_blocks = value_proj.reshape(blocks, BLOCK, HEADS, HEAD_DIM)
    query_blocks = query_proj.reshape(blocks, BLOCK, HEADS, HEAD_DIM)
    score_scale = HEAD_DIM ** -0.5

    def one_block(inputs):
        query_block, listed, block_index = inputs
        safe_index = jnp.maximum(listed, 0).astype(jnp.int32)
        keys_sel = key_blocks[safe_index].reshape(TOPK * BLOCK, HEADS, HEAD_DIM).astype(jnp.float32)
        values_sel = value_blocks[safe_index].reshape(TOPK * BLOCK, HEADS, HEAD_DIM).astype(jnp.float32)
        key_pos = (safe_index[:, None] * BLOCK + jnp.arange(BLOCK, dtype=jnp.int32)[None, :]).reshape(-1)
        key_valid = jnp.repeat(listed >= 0, BLOCK)
        query_pos = block_index * BLOCK + jnp.arange(BLOCK, dtype=jnp.int32)
        allowed = key_valid[None, :] & (key_pos[None, :] <= query_pos[:, None])
        scores = jnp.einsum("qhd,khd->hqk", query_block.astype(jnp.float32), keys_sel) * score_scale
        scores = jnp.where(allowed[None], scores, masked_score)
        peak_row = jnp.max(scores, axis=2, keepdims=True)
        weights = jnp.where(allowed[None], jnp.exp(scores - peak_row), 0.0)
        denominator = jnp.sum(weights, axis=2)
        weight_low = lax.optimization_barrier(weights.astype(jnp.bfloat16))
        summed = jnp.einsum("hqk,khd->qhd", weight_low.astype(jnp.float32), values_sel)
        return (summed / denominator.T[:, :, None]).astype(jnp.bfloat16)

    attended = lax.map(one_block, (query_blocks, chosen, jnp.arange(blocks, dtype=jnp.int32)))
    attended = attended.reshape(length, HEADS * HEAD_DIM)
    return jnp.dot(attended, out_weight, preferred_element_type=jnp.float32).astype(jnp.bfloat16)
```

```python
import functools

import jax
import jax.numpy as jnp
import numpy as np
from jax import lax
from jax.experimental import pallas as pl
from jax.experimental.pallas import tpu as pltpu
from jax.sharding import PartitionSpec as P

DP_KV = ("dp", "kv")
MESH = pl.DeviceIdType.MESH

HEAD_DIM = 64
BLOCK = 32
CAP = 3
ROWS = 256
QB = 8
XS = 4
ZS = 8
SRC = 8
PAIR = 128
LISTED = CAP * SRC * BLOCK
OUT_KEYS = SRC * BLOCK
HP = 4
SLOTS = 3
MASKED = -1e30
ROTARY_BASE = 500000.0


def tables():
    lane = np.arange(PAIR)
    inverse = ROTARY_BASE ** (-(lane % 32) / 32.0)
    inside = np.arange(ROWS)[:, None] * inverse[None, :]
    device = (np.arange(XS * ZS) * ROWS)[:, None] * inverse[None, :]
    row_table = np.stack([np.cos(inside), np.sin(inside)]).astype(np.float32)
    device_table = np.zeros((XS * ZS, 8, PAIR), np.float32)
    device_table[:, 0] = np.cos(device)
    device_table[:, 1] = np.sin(device)
    return row_table, device_table


def iota(shape, dim):
    return lax.broadcasted_iota(jnp.int32, shape, dim)


def half_scores(q, keys, half):
    q_half = q * half
    return lax.dot_general(
        q_half, keys, (((1,), (1,)), ((), ())), preferred_element_type=jnp.float32
    )


def attend(q, keys, values, bias):
    lane = iota((1, PAIR), 1)
    first = (lane < HEAD_DIM).astype(jnp.float32)
    halves = (first.astype(jnp.bfloat16), (1.0 - first).astype(jnp.bfloat16))
    outs, peaks = [], []
    for half, other in (halves, halves[::-1]):
        scores = half_scores(q, keys, half)
        scores = bias(scores)
        peak = jnp.max(scores, axis=1, keepdims=True)
        weight = jnp.exp(scores - peak).astype(jnp.bfloat16)
        outs.append(
            jnp.dot(weight, values * half + other, preferred_element_type=jnp.float32)
        )
        peaks.append(peak)
    in_first = iota((ROWS, PAIR), 1) < HEAD_DIM
    numerator = jnp.where(in_first, outs[0], outs[1])
    sums = pltpu.roll(jnp.where(in_first, outs[1], outs[0]), HEAD_DIM, 1)
    peak = jnp.where(in_first, peaks[0], peaks[1])
    return numerator, sums, peak


def compact(peak, sums):
    lane = iota((ROWS, PAIR), 1)
    turned = jnp.where(lane % HEAD_DIM < 32, peak, sums).T
    row = iota((8, ROWS), 0) % 4
    return jnp.where(
        row == 0,
        turned[0:8],
        jnp.where(row == 1, turned[32:40], jnp.where(row == 2, turned[64:72], turned[96:104])),
    )


def kernel(
    tok_hbm, wq_hbm, wk_hbm, wv_hbm, ow_hbm, ch_hbm, tab_hbm, dev_hbm, out_hbm, *scratch
):
    kv = scratch[:HP]
    (
        tok, wq, wk, wv, ow, ch, tab, dev, angle, acc, listing, own_bias, pair_bias, table,
        got_bias, got_table, q_buf, o_out, s_out, o_in, s_in, own_o, own_s, att, out_buf, small,
        load_sem, send, recv, tok_sem, q_send, q_recv, m_send, m_recv, o_send, o_recv,
        s_send, s_recv, small_sem, out_sem,
    ) = scratch[HP:]
    dp, me, core = (lax.axis_index(a) for a in ("dp", "kv", "tp"))
    z, x = me // XS, me % XS
    pair, odd = z // 2, z % 2
    left, right = (x + XS - 1) % XS, (x + 1) % XS
    other_row = z + 1 - 2 * odd
    half_d = tok.shape[2]
    width = wq.shape[1]

    def at(row, column):
        return (dp, row * XS + column, core)

    mate = (dp, me, 1 - core)

    loads = [
        (tok_hbm, tok.at[core]), (wk_hbm, wk), (wv_hbm, wv), (wq_hbm, wq), (ch_hbm, ch),
        (tab_hbm, tab), (dev_hbm, dev), (ow_hbm, ow),
    ]
    loads = [
        pltpu.make_async_copy(a, b, load_sem.at[i]) for i, (a, b) in enumerate(loads)
    ]
    for i in (4, 0, 1, 2, 3, 5, 6, 7):
        loads[i].start()

    barrier = pltpu.get_barrier_semaphore()

    def greet(device):
        pl.semaphore_signal(barrier, inc=1, device_id=device, device_id_type=MESH)

    greet(mate)
    greet(at(z, left))
    greet(at(z, right))
    for k in range(1, ZS):
        greet(at((z + k) % ZS, x))

    loads[4].wait()
    lane = iota((QB, ROWS), 1)
    lane8 = lane % QB
    chosen = ch[...]
    hit = jnp.zeros((QB, ROWS), jnp.int32)
    for t in range(chosen.shape[1]):
        hit = jnp.where(chosen[:, t : t + 1] == lane, 1, hit)
    need = jnp.max(hit, axis=0, keepdims=True)
    need = jnp.broadcast_to(need, (QB, ROWS))
    need = jnp.where(lane // QB == me, 0, need)
    rank = need
    for k in (1, 2, 4):
        rank = rank + jnp.where(lane8 >= k, pltpu.roll(rank, k, 1), 0)
    rank = rank - need
    sub = iota((QB, ROWS), 0)
    listed = jnp.zeros((QB, ROWS), jnp.int32)
    placed = []
    for slot in range(CAP):
        here = jnp.where(rank == slot, need, 0)
        placed.append((hit * here).astype(jnp.float32))
        where = here * lane8
        for k in (1, 2, 4):
            where = where + jnp.where(lane8 >= k, pltpu.roll(where, k, 1), 0)
        listed = jnp.where(sub == slot, where, listed)
    table[...] = listed
    placed = jnp.concatenate(placed, axis=0).astype(jnp.bfloat16)
    for k in range(4):
        spread = (iota((ROWS, OUT_KEYS), 0) // QB) == (iota((ROWS, OUT_KEYS), 1) // BLOCK + k * SRC)
        spread = spread.astype(jnp.float32).astype(jnp.bfloat16)
        found = jnp.dot(placed, spread, preferred_element_type=jnp.float32)
        pair_bias[k] = (found - 1.0) * -MASKED
    spread = iota((ROWS, ROWS), 0) == (iota((ROWS, ROWS), 1) // BLOCK + me * QB)
    spread = spread.astype(jnp.float32).astype(jnp.bfloat16)
    found = jnp.dot(
        hit.astype(jnp.float32).astype(jnp.bfloat16), spread, preferred_element_type=jnp.float32
    )
    listing[...] = (found - 1.0) * -MASKED
    for b in range(QB):
        rows = pl.ds(b * BLOCK, BLOCK)
        causal = iota((BLOCK, ROWS), 1) <= iota((BLOCK, ROWS), 0) + b * BLOCK
        own_bias[rows, :] = jnp.where(causal, listing[b : b + 1, :], MASKED)

    loads[5].wait()
    loads[6].wait()
    dev_cos, dev_sin = dev[me, 0:1, :], dev[me, 1:2, :]
    sign = jnp.where(iota((1, PAIR), 1) % HEAD_DIM < 32, -1.0, 1.0)
    angle[0] = tab[0] * dev_cos - tab[1] * dev_sin
    angle[1] = (tab[1] * dev_cos + tab[0] * dev_sin) * sign

    for k in range(SLOTS):
        @pl.when(pair <= k)
        def _():
            for hp in range(HP):
                o_in[hp, k] = jnp.zeros((ROWS, PAIR), jnp.bfloat16)
                s_in[hp, k] = jnp.full((8, ROWS), MASKED, jnp.float32)

    def remote(src, dst, send_sem, recv_sem, device):
        return pltpu.make_async_remote_copy(
            src_ref=src, dst_ref=dst, send_sem=send_sem, recv_sem=recv_sem,
            device_id=device, device_id_type=MESH,
        )

    pl.semaphore_wait(barrier, 3 + ZS - 1)
    loads[0].wait()
    tokens = remote(tok.at[core], tok.at[core], tok_sem.at[0], tok_sem.at[1], mate)
    tokens.start()

    for w, load in ((0, 1), (1, 2), (2, 3)):
        loads[load].wait()
        weight = (wk, wv, wq)[w]
        for c in range(width // 256):
            cols = pl.ds(c * 256, 256)
            acc[w, c] = jnp.dot(
                tok[core], weight[pl.ds(core * half_d, half_d), cols],
                preferred_element_type=jnp.float32,
            )
    theirs = remote(tok.at[1 - core], tok.at[1 - core], tok_sem.at[0], tok_sem.at[1], mate)
    theirs.wait_recv()

    def project(w, c):
        weight = (wk, wv, wq)[w]
        cols = pl.ds(c * 256, 256)
        return acc[w, c] + jnp.dot(
            tok[1 - core], weight[pl.ds((1 - core) * half_d, half_d), cols],
            preferred_element_type=jnp.float32,
        )

    low = iota((ROWS, PAIR), 1) % HEAD_DIM < 32

    def turn(part):
        partner = jnp.where(low, pltpu.roll(part, PAIR - 32, 1), pltpu.roll(part, 32, 1))
        return part * angle[0] + partner * angle[1]

    def blocked(part):
        return part.astype(jnp.bfloat16).reshape(QB, BLOCK, PAIR)

    own = odd * XS + x
    mated = (1 - odd) * XS + x
    far = (x + 2) % XS

    def hop(kind, hp, source, device, which=None):
        part = kv[hp].at[source] if which is None else kv[hp].at[source, which]
        return remote(part, part, send.at[kind, hp], recv.at[kind, hp], device)

    def send_own(hp):
        hop(1, hp, own, at(z, right)).start()
        hop(2, hp, own, at(z, left)).start()

    def send_across(hp):
        hop(0, hp, own, at(other_row, x)).start()

    q_row = [1 - z // 5, 3 - z // 7, z * 0 + 5]
    q_slot = [(z + 1) % 3, (z + 2) % 3, z % 2]

    def q_copy(k, hp, slot):
        return remote(
            q_buf.at[hp, SLOTS], q_buf.at[hp, slot], q_send.at[k, hp], q_recv.at[slot, hp],
            at(q_row[k], x),
        )

    def meta_copies(k, slot):
        return (
            remote(pair_bias.at[k], got_bias.at[slot], m_send.at[k, 0], m_recv.at[slot, 0],
                   at(q_row[k], x)),
            remote(table, got_table.at[slot], m_send.at[k, 1], m_recv.at[slot, 1],
                   at(q_row[k], x)),
        )

    for c in range(width // 256):
        keys, values = project(0, c), project(1, c)
        for i in range(2):
            hp = 2 * c + i
            part = slice(i * PAIR, (i + 1) * PAIR)
            kv[hp][own, 0] = blocked(turn(keys[:, part]))
            kv[hp][own, 1] = blocked(values[:, part])
            send_across(hp)
            if hp < 2:
                send_own(hp)
    for c in range(width // 256):
        queries = project(2, c)
        for i in range(2):
            hp = 2 * c + i
            part = slice(i * PAIR, (i + 1) * PAIR)
            turned = turn(queries[:, part]).astype(jnp.bfloat16).astype(jnp.float32)
            q_buf[hp, SLOTS] = (turned * HEAD_DIM**-0.5).astype(jnp.bfloat16)
            for k in range(SLOTS):
                @pl.when(pair > k)
                def _():
                    if hp == 0:
                        for copy in meta_copies(k, q_slot[k]):
                            copy.start()
                    q_copy(k, hp, q_slot[k]).start()

    own_small = pltpu.make_async_copy(table, small.at[SLOTS], small_sem.at[SLOTS])
    own_small.start()

    own_left, own_right, own_far = odd * XS + left, odd * XS + right, odd * XS + far
    row2 = (1 - odd) * XS
    mate_left, mate_right, mate_far = row2 + left, row2 + right, row2 + far

    def pass_mate(hp):
        hop(0, hp, mated, at(other_row, x)).wait_recv()
        hop(3, hp, mated, at(z, right)).start()
        hop(4, hp, mated, at(z, left)).start()

    def relay_own(hp):
        hop(1, hp, own_left, at(z, right)).wait_recv()
        hop(5, hp, own_left, at(z, right), 0).start()
        hop(2, hp, own_right, at(z, left)).wait_recv()
        hop(6, hp, own_right, at(z, left), 1).start()

    def relay_mate(hp):
        hop(3, hp, mate_left, at(z, right)).wait_recv()
        hop(7, hp, mate_left, at(z, right), 0).start()
        hop(4, hp, mate_right, at(z, left)).wait_recv()
        hop(8, hp, mate_right, at(z, left), 1).start()

    def complete(hp):
        hop(5, hp, own_far, at(z, right), 0).wait_recv()
        hop(6, hp, own_far, at(z, left), 1).wait_recv()
        hop(7, hp, mate_far, at(z, right), 0).wait_recv()
        hop(8, hp, mate_far, at(z, left), 1).wait_recv()

    def gathered(hp, slot, which):
        blocks = []
        for k in range(CAP):
            for s in range(SRC):
                index = small[slot, k, pair * (QB * SRC) + s * QB + QB - 1]
                blocks.append(kv[hp][s, which, index])
        return blocks

    def wide_bias(bias):
        return jnp.concatenate([bias[k * QB : (k + 1) * QB] for k in range(CAP)], axis=1)

    base = 5 + 2 * pair - 3 * odd

    def partial_copies(hp, slot, k):
        row = base + slot
        return (
            remote(o_out.at[hp, slot], o_in.at[hp, k], o_send.at[slot, hp], o_recv.at[k, hp],
                   at(row, x)),
            remote(s_out.at[hp, slot], s_in.at[hp, k], s_send.at[slot, hp], s_recv.at[k, hp],
                   at(row, x)),
        )

    def visitors(hp):
        @pl.loop(0, SLOTS)
        def _(slot):
            @pl.when(base + slot < ZS)
            def _():
                if hp == 0:
                    for ref, i in ((got_bias, 0), (got_table, 1)):
                        remote(ref.at[slot], ref.at[slot], m_send.at[0, i], m_recv.at[slot, i],
                               mate).wait_recv()
                    copy = pltpu.make_async_copy(
                        got_table.at[slot], small.at[slot], small_sem.at[slot]
                    )
                    copy.start()
                    copy.wait()
                q_ref = q_buf.at[hp, slot]
                remote(q_ref, q_ref, q_send.at[0, hp], q_recv.at[slot, hp], mate).wait_recv()
                keys = jnp.concatenate(gathered(hp, slot, 0), axis=0)
                values = jnp.concatenate(gathered(hp, slot, 1), axis=0)
                bias = wide_bias(got_bias[slot])

                def masked(scores):
                    scores = scores.reshape(QB, BLOCK, LISTED) + bias[:, None, :]
                    return scores.reshape(ROWS, LISTED)

                numerator, sums, peak = attend(q_ref[...], keys, values, masked)
                o_out[hp, slot] = (numerator / sums).astype(jnp.bfloat16)
                s_out[hp, slot] = compact(peak, sums)
                for copy in partial_copies(hp, slot, pair):
                    copy.start()

    def own_queries(hp):
        if hp == 0:
            own_small.wait()
        keys = jnp.concatenate(gathered(hp, SLOTS, 0) + [kv[hp][own, 0].reshape(ROWS, PAIR)], axis=0)
        values = jnp.concatenate(gathered(hp, SLOTS, 1) + [kv[hp][own, 1].reshape(ROWS, PAIR)], axis=0)
        bias = wide_bias(pair_bias[pair])

        def masked(scores):
            others = scores[:, :LISTED].reshape(QB, BLOCK, LISTED) + bias[:, None, :]
            mine = scores[:, LISTED:] + own_bias[...]
            return jnp.concatenate([others.reshape(ROWS, LISTED), mine], axis=1)

        numerator, sums, peak = attend(q_buf[hp, SLOTS], keys, values, masked)
        own_o[hp] = numerator / sums
        own_s[hp] = compact(peak, sums)

    def att_copy(hp, side):
        part = att.at[side, hp]
        return remote(part, part, send.at[9, hp], recv.at[9, hp], mate)

    def merge(hp):
        for k in range(SLOTS):
            @pl.when(pair > k)
            def _():
                for ref, sem in ((o_in, o_recv), (s_in, s_recv)):
                    part = ref.at[hp, k]
                    remote(part, part, o_send.at[0, hp], sem.at[k, hp], mate).wait_recv()
        stats = [own_s[hp]] + [s_in[hp, k] for k in range(SLOTS)]
        shares = [[None, None] for _ in stats]
        for h in range(2):
            peaks = [s[2 * h : 2 * h + 1] for s in stats]
            top = functools.reduce(jnp.maximum, peaks)
            weights = [
                s[2 * h + 1 : 2 * h + 2] * jnp.exp(p - top) for s, p in zip(stats, peaks)
            ]
            scale = 1.0 / functools.reduce(jnp.add, weights)
            for i, w in enumerate(weights):
                shares[i][h] = w * scale
        rows = [jnp.broadcast_to(s, (16, ROWS)) for share in shares for s in share]
        turned = jnp.concatenate(rows, axis=0).T
        in_first = iota((ROWS, PAIR), 1) < HEAD_DIM
        total = jnp.zeros((ROWS, PAIR), jnp.float32)
        for i in range(1 + SLOTS):
            share = jnp.where(
                in_first, turned[:, i * 32 : i * 32 + 1], turned[:, i * 32 + 16 : i * 32 + 17]
            )
            part = own_o[hp] if i == 0 else o_in[hp, i - 1].astype(jnp.float32)
            total = total + share * part
        att[core, hp] = total.astype(jnp.bfloat16)
        att_copy(hp, core).start()

    pass_mate(0)
    relay_own(0)
    send_own(2)
    relay_mate(0)
    pass_mate(1)
    relay_own(1)
    send_own(3)
    for hp in range(HP):
        complete(hp)
        visitors(hp)
        if hp + 1 < HP:
            relay_mate(hp + 1)
        if hp + 2 < HP:
            pass_mate(hp + 2)
            relay_own(hp + 2)
        own_queries(hp)
        if hp:
            merge(hp - 1)
    merge(HP - 1)

    for hp in range(HP):
        att_copy(hp, 1 - core).wait_recv()
    loads[7].wait()
    attended = jnp.concatenate([att[s, hp] for s in range(2) for hp in range(HP)], axis=1)
    stores = []
    for c in range(ow.shape[1] // 256):
        cols = pl.ds(c * 256, 256)
        out_buf[:, cols] = jnp.dot(
            attended, ow[:, cols], preferred_element_type=jnp.float32
        ).astype(jnp.bfloat16)
        store = pltpu.make_async_copy(
            out_buf.at[:, cols], out_hbm.at[:, cols], out_sem.at[c]
        )
        store.start()
        stores.append(store)

    tokens.wait_send()
    for hp in range(HP):
        hop(0, hp, own, at(other_row, x)).wait_send()
        hop(1, hp, own, at(z, right)).wait_send()
        hop(2, hp, own, at(z, left)).wait_send()
        hop(3, hp, mated, at(z, right)).wait_send()
        hop(4, hp, mated, at(z, left)).wait_send()
        hop(5, hp, own_left, at(z, right), 0).wait_send()
        hop(6, hp, own_right, at(z, left), 1).wait_send()
        hop(7, hp, mate_left, at(z, right), 0).wait_send()
        hop(8, hp, mate_right, at(z, left), 1).wait_send()
        att_copy(hp, core).wait_send()
    for k in range(SLOTS):
        @pl.when(pair > k)
        def _():
            for copy in meta_copies(k, q_slot[k]):
                copy.wait_send()
            for hp in range(HP):
                q_copy(k, hp, q_slot[k]).wait_send()

    @pl.loop(0, SLOTS)
    def _(slot):
        @pl.when(base + slot < ZS)
        def _():
            for hp in range(HP):
                for copy in partial_copies(hp, slot, pair):
                    copy.wait_send()

    for store in stores:
        store.wait()


def on_device(tokens, query_weight, key_weight, value_weight, out_weight, chosen):
    rows, half_d = tokens.shape
    width = query_weight.shape[1]
    out_half = out_weight.shape[1]
    row_table, device_table = tables()
    bf16, f32, i32 = jnp.bfloat16, jnp.float32, jnp.int32
    vmem = pltpu.VMEM
    dma = pltpu.SemaphoreType.DMA
    scratch = [vmem((SRC, 2, QB, BLOCK, PAIR), bf16) for _ in range(HP)] + [
        vmem((2, rows, half_d), bf16),
        vmem(query_weight.shape, bf16),
        vmem(key_weight.shape, bf16),
        vmem(value_weight.shape, bf16),
        vmem(out_weight.shape, bf16),
        vmem(chosen.shape, i32),
        vmem(row_table.shape, f32),
        vmem(device_table.shape, f32),
        vmem((2, ROWS, PAIR), f32),
        vmem((3, width // 256, ROWS, 256), f32),
        vmem((QB, ROWS), f32),
        vmem((ROWS, ROWS), f32),
        vmem((4, CAP * QB, OUT_KEYS), f32),
        vmem((QB, ROWS), i32),
        vmem((SLOTS, CAP * QB, OUT_KEYS), f32),
        vmem((SLOTS, QB, ROWS), i32),
        vmem((HP, SLOTS + 1, ROWS, PAIR), bf16),
        vmem((HP, SLOTS, ROWS, PAIR), bf16),
        vmem((HP, SLOTS, 8, ROWS), f32),
        vmem((HP, SLOTS, ROWS, PAIR), bf16),
        vmem((HP, SLOTS, 8, ROWS), f32),
        vmem((HP, ROWS, PAIR), f32),
        vmem((HP, 8, ROWS), f32),
        vmem((2, HP, ROWS, PAIR), bf16),
        vmem((rows, out_half), bf16),
        pltpu.SMEM((SLOTS + 1, QB, ROWS), i32),
        dma((8,)),
        dma((10, HP)),
        dma((10, HP)),
        dma((2,)),
        dma((SLOTS, HP)),
        dma((SLOTS, HP)),
        dma((SLOTS, 2)),
        dma((SLOTS, 2)),
        dma((SLOTS, HP)),
        dma((SLOTS, HP)),
        dma((SLOTS, HP)),
        dma((SLOTS, HP)),
        dma((SLOTS + 1,)),
        dma((out_half // 256,)),
    ]
    return pl.pallas_call(
        kernel,
        out_shape=jax.ShapeDtypeStruct((rows, out_half), bf16),
        in_specs=[pl.BlockSpec(memory_space=pl.ANY)] * 8,
        out_specs=pl.BlockSpec(memory_space=pl.ANY),
        scratch_shapes=scratch,
        compiler_params=pltpu.CompilerParams(
            collective_id=0, has_side_effects=True, vmem_limit_bytes=58 * 1024 * 1024
        ),
        name="block_attention",
    )(
        tokens, query_weight, key_weight, value_weight, out_weight, chosen,
        jnp.asarray(row_table), jnp.asarray(device_table),
    )


def solution(mesh):
    placed = (
        P(DP_KV, "tp"),
        P(None, "tp"),
        P(None, "tp"),
        P(None, "tp"),
        P(None, "tp"),
        P(DP_KV, None),
    )
    return jax.shard_map(
        on_device, mesh=mesh, in_specs=placed, out_specs=P(DP_KV, "tp"), check_vma=False
    )
```

```python
import functools

import jax
import jax.numpy as jnp
import numpy as np
from jax import lax
from jax.experimental import pallas as pl
from jax.experimental.pallas import tpu as pltpu
from jax.sharding import PartitionSpec as P

DP_KV = ("dp", "kv")
MESH = pl.DeviceIdType.MESH

HEAD_DIM = 64
BLOCK = 32
CAP = 3
ROWS = 256
QB = 8
XS = 4
ZS = 8
SRC = 8
PAIR = 128
LISTED = CAP * SRC * BLOCK
OUT_KEYS = SRC * BLOCK
HP = 4
SLOTS = 3
MASKED = -1e30
ROTARY_BASE = 500000.0


def tables():
    lane = np.arange(PAIR)
    inverse = ROTARY_BASE ** (-(lane % 32) / 32.0)
    inside = np.arange(ROWS)[:, None] * inverse[None, :]
    device = (np.arange(XS * ZS) * ROWS)[:, None] * inverse[None, :]
    row_table = np.stack([np.cos(inside), np.sin(inside)]).astype(np.float32)
    device_table = np.zeros((XS * ZS, 8, PAIR), np.float32)
    device_table[:, 0] = np.cos(device)
    device_table[:, 1] = np.sin(device)
    return row_table, device_table


def iota(shape, dim):
    return lax.broadcasted_iota(jnp.int32, shape, dim)


def half_scores(q, keys, half):
    q_half = q * half
    return lax.dot_general(
        q_half, keys, (((1,), (1,)), ((), ())), preferred_element_type=jnp.float32
    )


def attend(q, keys, values, bias):
    lane = iota((1, PAIR), 1)
    first = (lane < HEAD_DIM).astype(jnp.float32)
    halves = (first.astype(jnp.bfloat16), (1.0 - first).astype(jnp.bfloat16))
    outs, peaks = [], []
    for half, other in (halves, halves[::-1]):
        scores = half_scores(q, keys, half)
        scores = bias(scores)
        peak = jnp.max(scores, axis=1, keepdims=True)
        weight = jnp.exp(scores - peak).astype(jnp.bfloat16)
        outs.append(
            jnp.dot(weight, values * half + other, preferred_element_type=jnp.float32)
        )
        peaks.append(peak)
    in_first = iota((ROWS, PAIR), 1) < HEAD_DIM
    numerator = jnp.where(in_first, outs[0], outs[1])
    sums = pltpu.roll(jnp.where(in_first, outs[1], outs[0]), HEAD_DIM, 1)
    peak = jnp.where(in_first, peaks[0], peaks[1])
    return numerator, sums, peak


def compact(peak, sums):
    lane = iota((ROWS, PAIR), 1)
    turned = jnp.where(lane % HEAD_DIM < 32, peak, sums).T
    row = iota((8, ROWS), 0) % 4
    return jnp.where(
        row == 0,
        turned[0:8],
        jnp.where(row == 1, turned[32:40], jnp.where(row == 2, turned[64:72], turned[96:104])),
    )


def kernel(
    tok_hbm, wq_hbm, wk_hbm, wv_hbm, ow_hbm, ch_hbm, tab_hbm, dev_hbm, out_hbm, *scratch
):
    kv = scratch[:HP]
    (
        tok, wq, wk, wv, ow, ch, tab, dev, angle, acc, listing, own_bias, pair_bias, table,
        got_bias, got_table, q_buf, o_out, s_out, o_in, s_in, own_o, own_s, att, out_buf, out_acc, small,
        load_sem, send, recv, tok_sem, q_send, q_recv, m_send, m_recv, o_send, o_recv,
        s_send, s_recv, small_sem, out_sem,
    ) = scratch[HP:]
    dp, me, core = (lax.axis_index(a) for a in ("dp", "kv", "tp"))
    z, x = me // XS, me % XS
    pair, odd = z // 2, z % 2
    left, right = (x + XS - 1) % XS, (x + 1) % XS
    other_row = z + 1 - 2 * odd
    half_d = tok.shape[2]
    width = wq.shape[1]

    def at(row, column):
        return (dp, row * XS + column, core)

    mate = (dp, me, 1 - core)

    loads = [
        (tok_hbm, tok.at[core]), (wk_hbm, wk), (wv_hbm, wv), (wq_hbm, wq), (ch_hbm, ch),
        (tab_hbm, tab), (dev_hbm, dev), (ow_hbm, ow),
    ]
    loads = [
        pltpu.make_async_copy(a, b, load_sem.at[i]) for i, (a, b) in enumerate(loads)
    ]
    for i in (0, 1, 2, 3, 5, 6, 4, 7):
        loads[i].start()

    barrier = pltpu.get_barrier_semaphore()

    def greet(device):
        pl.semaphore_signal(barrier, inc=1, device_id=device, device_id_type=MESH)

    greet(mate)
    greet(at(z, left))
    greet(at(z, right))
    for k in range(1, ZS):
        greet(at((z + k) % ZS, x))

    loads[5].wait()
    loads[6].wait()
    dev_cos, dev_sin = dev[me, 0:1, :], dev[me, 1:2, :]
    sign = jnp.where(iota((1, PAIR), 1) % HEAD_DIM < 32, -1.0, 1.0)
    angle[0] = tab[0] * dev_cos - tab[1] * dev_sin
    angle[1] = (tab[1] * dev_cos + tab[0] * dev_sin) * sign

    def remote(src, dst, send_sem, recv_sem, device):
        return pltpu.make_async_remote_copy(
            src_ref=src, dst_ref=dst, send_sem=send_sem, recv_sem=recv_sem,
            device_id=device, device_id_type=MESH,
        )

    loads[0].wait()
    for w, load in ((0, 1), (1, 2), (2, 3)):
        loads[load].wait()
        weight = (wk, wv, wq)[w]
        for c in range(width // 256):
            cols = pl.ds(c * 256, 256)
            acc[w, c] = jnp.dot(
                tok[core], weight[pl.ds(core * half_d, half_d), cols],
                preferred_element_type=jnp.float32,
            )
    pl.semaphore_wait(barrier, 3 + ZS - 1)
    tokens = remote(tok.at[core], tok.at[core], tok_sem.at[0], tok_sem.at[1], mate)
    tokens.start()

    loads[4].wait()
    lane = iota((QB, ROWS), 1)
    lane8 = lane % QB
    chosen = ch[...]
    hit = jnp.zeros((QB, ROWS), jnp.int32)
    for t in range(chosen.shape[1]):
        hit = jnp.where(chosen[:, t : t + 1] == lane, 1, hit)
    need = jnp.max(hit, axis=0, keepdims=True)
    need = jnp.broadcast_to(need, (QB, ROWS))
    need = jnp.where(lane // QB == me, 0, need)
    rank = need
    for k in (1, 2, 4):
        rank = rank + jnp.where(lane8 >= k, pltpu.roll(rank, k, 1), 0)
    rank = rank - need
    sub = iota((QB, ROWS), 0)
    listed = jnp.zeros((QB, ROWS), jnp.int32)
    placed = []
    for slot in range(CAP):
        here = jnp.where(rank == slot, need, 0)
        placed.append((hit * here).astype(jnp.float32))
        where = here * lane8
        for k in (1, 2, 4):
            where = where + jnp.where(lane8 >= k, pltpu.roll(where, k, 1), 0)
        listed = jnp.where(sub == slot, where, listed)
    table[...] = listed
    placed = jnp.concatenate(placed, axis=0).astype(jnp.bfloat16)
    for k in range(4):
        spread = (iota((ROWS, OUT_KEYS), 0) // QB) == (iota((ROWS, OUT_KEYS), 1) // BLOCK + k * SRC)
        spread = spread.astype(jnp.float32).astype(jnp.bfloat16)
        found = jnp.dot(placed, spread, preferred_element_type=jnp.float32)
        pair_bias[k] = (found - 1.0) * -MASKED
    spread = iota((ROWS, ROWS), 0) == (iota((ROWS, ROWS), 1) // BLOCK + me * QB)
    spread = spread.astype(jnp.float32).astype(jnp.bfloat16)
    found = jnp.dot(
        hit.astype(jnp.float32).astype(jnp.bfloat16), spread, preferred_element_type=jnp.float32
    )
    listing[...] = (found - 1.0) * -MASKED
    for b in range(QB):
        rows = pl.ds(b * BLOCK, BLOCK)
        causal = iota((BLOCK, ROWS), 1) <= iota((BLOCK, ROWS), 0) + b * BLOCK
        own_bias[rows, :] = jnp.where(causal, listing[b : b + 1, :], MASKED)

    for k in range(SLOTS):
        @pl.when(pair <= k)
        def _():
            for hp in range(HP):
                o_in[hp, k] = jnp.zeros((ROWS, PAIR), jnp.bfloat16)
                s_in[hp, k] = jnp.full((8, ROWS), MASKED, jnp.float32)

    theirs = remote(tok.at[1 - core], tok.at[1 - core], tok_sem.at[0], tok_sem.at[1], mate)
    theirs.wait_recv()

    def project(w, c):
        weight = (wk, wv, wq)[w]
        cols = pl.ds(c * 256, 256)
        return acc[w, c] + jnp.dot(
            tok[1 - core], weight[pl.ds((1 - core) * half_d, half_d), cols],
            preferred_element_type=jnp.float32,
        )

    low = iota((ROWS, PAIR), 1) % HEAD_DIM < 32

    def turn(part):
        partner = jnp.where(low, pltpu.roll(part, PAIR - 32, 1), pltpu.roll(part, 32, 1))
        return part * angle[0] + partner * angle[1]

    def blocked(part):
        return part.astype(jnp.bfloat16).reshape(QB, BLOCK, PAIR)

    own = odd * XS + x
    mated = (1 - odd) * XS + x
    far = (x + 2) % XS

    def hop(kind, hp, source, device, which=None):
        part = kv[hp].at[source] if which is None else kv[hp].at[source, which]
        return remote(part, part, send.at[kind, hp], recv.at[kind, hp], device)

    def send_own(hp):
        hop(1, hp, own, at(z, right)).start()
        hop(2, hp, own, at(z, left)).start()

    def send_across(hp):
        hop(0, hp, own, at(other_row, x)).start()

    q_row = [1 - z // 5, 3 - z // 7, z * 0 + 5]
    q_slot = [(z + 1) % 3, (z + 2) % 3, z % 2]

    def q_copy(k, hp, slot):
        return remote(
            q_buf.at[hp, SLOTS], q_buf.at[hp, slot], q_send.at[k, hp], q_recv.at[slot, hp],
            at(q_row[k], x),
        )

    def meta_copies(k, slot):
        return (
            remote(pair_bias.at[k], got_bias.at[slot], m_send.at[k, 0], m_recv.at[slot, 0],
                   at(q_row[k], x)),
            remote(table, got_table.at[slot], m_send.at[k, 1], m_recv.at[slot, 1],
                   at(q_row[k], x)),
        )

    def send_queries(hp):
        for k in range(SLOTS):
            @pl.when(pair > k)
            def _():
                if hp == 0:
                    for copy in meta_copies(k, q_slot[k]):
                        copy.start()
                q_copy(k, hp, q_slot[k]).start()

    for c in range(width // 256):
        keys, values = project(0, c), project(1, c)
        for i in range(2):
            hp = 2 * c + i
            part = slice(i * PAIR, (i + 1) * PAIR)
            kv[hp][own, 0] = blocked(turn(keys[:, part]))
            kv[hp][own, 1] = blocked(values[:, part])
            if i == 0:
                send_across(hp)
            if c == 0:
                send_own(hp)
        queries = project(2, c)
        for i in range(2):
            hp = 2 * c + i
            part = slice(i * PAIR, (i + 1) * PAIR)
            turned = turn(queries[:, part]).astype(jnp.bfloat16).astype(jnp.float32)
            q_buf[hp, SLOTS] = (turned * HEAD_DIM**-0.5).astype(jnp.bfloat16)
            send_queries(hp)
            if i == 0:
                send_across(hp + 1)

    own_small = pltpu.make_async_copy(table, small.at[SLOTS], small_sem.at[SLOTS])
    own_small.start()

    own_left, own_right, own_far = odd * XS + left, odd * XS + right, odd * XS + far
    row2 = (1 - odd) * XS
    mate_left, mate_right, mate_far = row2 + left, row2 + right, row2 + far

    def pass_mate(hp):
        hop(0, hp, mated, at(other_row, x)).wait_recv()
        hop(3, hp, mated, at(z, right)).start()
        hop(4, hp, mated, at(z, left)).start()

    def relay_own(hp):
        hop(1, hp, own_left, at(z, right)).wait_recv()
        hop(5, hp, own_left, at(z, right), 0).start()
        hop(2, hp, own_right, at(z, left)).wait_recv()
        hop(6, hp, own_right, at(z, left), 1).start()

    def relay_mate(hp):
        hop(3, hp, mate_left, at(z, right)).wait_recv()
        hop(7, hp, mate_left, at(z, right), 0).start()
        hop(4, hp, mate_right, at(z, left)).wait_recv()
        hop(8, hp, mate_right, at(z, left), 1).start()

    def complete(hp):
        hop(5, hp, own_far, at(z, right), 0).wait_recv()
        hop(6, hp, own_far, at(z, left), 1).wait_recv()
        hop(7, hp, mate_far, at(z, right), 0).wait_recv()
        hop(8, hp, mate_far, at(z, left), 1).wait_recv()

    def gathered(hp, slot, which):
        blocks = []
        for k in range(CAP):
            for s in range(SRC):
                index = small[slot, k, pair * (QB * SRC) + s * QB + QB - 1]
                blocks.append(kv[hp][s, which, index])
        return blocks

    def wide_bias(bias):
        return jnp.concatenate([bias[k * QB : (k + 1) * QB] for k in range(CAP)], axis=1)

    base = 5 + 2 * pair - 3 * odd

    def partial_copies(hp, slot, k):
        row = base + slot
        return (
            remote(o_out.at[hp, slot], o_in.at[hp, k], o_send.at[slot, hp], o_recv.at[k, hp],
                   at(row, x)),
            remote(s_out.at[hp, slot], s_in.at[hp, k], s_send.at[slot, hp], s_recv.at[k, hp],
                   at(row, x)),
        )

    def visitors(hp):
        @pl.loop(0, SLOTS)
        def _(slot):
            @pl.when(base + slot < ZS)
            def _():
                if hp == 0:
                    for ref, i in ((got_bias, 0), (got_table, 1)):
                        remote(ref.at[slot], ref.at[slot], m_send.at[0, i], m_recv.at[slot, i],
                               mate).wait_recv()
                    copy = pltpu.make_async_copy(
                        got_table.at[slot], small.at[slot], small_sem.at[slot]
                    )
                    copy.start()
                    copy.wait()
                q_ref = q_buf.at[hp, slot]
                remote(q_ref, q_ref, q_send.at[0, hp], q_recv.at[slot, hp], mate).wait_recv()
                keys = jnp.concatenate(gathered(hp, slot, 0), axis=0)
                values = jnp.concatenate(gathered(hp, slot, 1), axis=0)
                bias = wide_bias(got_bias[slot])

                def masked(scores):
                    scores = scores.reshape(QB, BLOCK, LISTED) + bias[:, None, :]
                    return scores.reshape(ROWS, LISTED)

                numerator, sums, peak = attend(q_ref[...], keys, values, masked)
                o_out[hp, slot] = (numerator / sums).astype(jnp.bfloat16)
                s_out[hp, slot] = compact(peak, sums)
                for copy in partial_copies(hp, slot, pair):
                    copy.start()

    def own_queries(hp):
        if hp == 0:
            own_small.wait()
        keys = jnp.concatenate(gathered(hp, SLOTS, 0) + [kv[hp][own, 0].reshape(ROWS, PAIR)], axis=0)
        values = jnp.concatenate(gathered(hp, SLOTS, 1) + [kv[hp][own, 1].reshape(ROWS, PAIR)], axis=0)
        bias = wide_bias(pair_bias[pair])

        def masked(scores):
            others = scores[:, :LISTED].reshape(QB, BLOCK, LISTED) + bias[:, None, :]
            mine = scores[:, LISTED:] + own_bias[...]
            return jnp.concatenate([others.reshape(ROWS, LISTED), mine], axis=1)

        numerator, sums, peak = attend(q_buf[hp, SLOTS], keys, values, masked)
        own_o[hp] = numerator / sums
        own_s[hp] = compact(peak, sums)

    def att_copy(hp, side):
        part = att.at[side, hp]
        return remote(part, part, send.at[9, hp], recv.at[9, hp], mate)

    def merge(hp):
        for k in range(SLOTS):
            @pl.when(pair > k)
            def _():
                for ref, sem in ((o_in, o_recv), (s_in, s_recv)):
                    part = ref.at[hp, k]
                    remote(part, part, o_send.at[0, hp], sem.at[k, hp], mate).wait_recv()
        stats = [own_s[hp]] + [s_in[hp, k] for k in range(SLOTS)]
        shares = [[None, None] for _ in stats]
        for h in range(2):
            peaks = [s[2 * h : 2 * h + 1] for s in stats]
            top = functools.reduce(jnp.maximum, peaks)
            weights = [
                s[2 * h + 1 : 2 * h + 2] * jnp.exp(p - top) for s, p in zip(stats, peaks)
            ]
            scale = 1.0 / functools.reduce(jnp.add, weights)
            for i, w in enumerate(weights):
                shares[i][h] = w * scale
        rows = [jnp.broadcast_to(s, (16, ROWS)) for share in shares for s in share]
        turned = jnp.concatenate(rows, axis=0).T
        in_first = iota((ROWS, PAIR), 1) < HEAD_DIM
        total = jnp.zeros((ROWS, PAIR), jnp.float32)
        for i in range(1 + SLOTS):
            share = jnp.where(
                in_first, turned[:, i * 32 : i * 32 + 1], turned[:, i * 32 + 16 : i * 32 + 17]
            )
            part = own_o[hp] if i == 0 else o_in[hp, i - 1].astype(jnp.float32)
            total = total + share * part
        att[core, hp] = total.astype(jnp.bfloat16)
        att_copy(hp, core).start()

    def project_out(hp):
        att_copy(hp, 1 - core).wait_recv()
        if hp == 0:
            loads[7].wait()
        heads = jnp.concatenate([att[s, hp] for s in range(2)], axis=1)
        outs = []
        for c in range(ow.shape[1] // 256):
            cols = pl.ds(c * 256, 256)
            weight = jnp.concatenate(
                [ow[pl.ds(s * width + hp * PAIR, PAIR), cols] for s in range(2)], axis=0
            )
            out = jnp.dot(heads, weight, preferred_element_type=jnp.float32)
            if hp:
                out = out + out_acc[c]
            if hp < HP - 1:
                out_acc[c] = out
            outs.append(out)
        return outs

    pass_mate(0)
    relay_own(0)
    send_own(2)
    relay_mate(0)
    pass_mate(1)
    relay_own(1)
    send_own(3)
    for hp in range(HP):
        complete(hp)
        visitors(hp)
        if hp + 1 < HP:
            relay_mate(hp + 1)
        if hp + 2 < HP:
            pass_mate(hp + 2)
            relay_own(hp + 2)
        own_queries(hp)
        if hp:
            merge(hp - 1)
        if hp > 1:
            project_out(hp - 2)
    merge(HP - 1)
    project_out(HP - 2)

    stores = []
    for c, out in enumerate(project_out(HP - 1)):
        cols = pl.ds(c * 256, 256)
        out_buf[:, cols] = out.astype(jnp.bfloat16)
        store = pltpu.make_async_copy(
            out_buf.at[:, cols], out_hbm.at[:, cols], out_sem.at[c]
        )
        store.start()
        stores.append(store)

    tokens.wait_send()
    for hp in range(HP):
        hop(0, hp, own, at(other_row, x)).wait_send()
        hop(1, hp, own, at(z, right)).wait_send()
        hop(2, hp, own, at(z, left)).wait_send()
        hop(3, hp, mated, at(z, right)).wait_send()
        hop(4, hp, mated, at(z, left)).wait_send()
        hop(5, hp, own_left, at(z, right), 0).wait_send()
        hop(6, hp, own_right, at(z, left), 1).wait_send()
        hop(7, hp, mate_left, at(z, right), 0).wait_send()
        hop(8, hp, mate_right, at(z, left), 1).wait_send()
        att_copy(hp, core).wait_send()
    for k in range(SLOTS):
        @pl.when(pair > k)
        def _():
            for copy in meta_copies(k, q_slot[k]):
                copy.wait_send()
            for hp in range(HP):
                q_copy(k, hp, q_slot[k]).wait_send()

    @pl.loop(0, SLOTS)
    def _(slot):
        @pl.when(base + slot < ZS)
        def _():
            for hp in range(HP):
                for copy in partial_copies(hp, slot, pair):
                    copy.wait_send()

    for store in stores:
        store.wait()


def on_device(tokens, query_weight, key_weight, value_weight, out_weight, chosen):
    rows, half_d = tokens.shape
    width = query_weight.shape[1]
    out_half = out_weight.shape[1]
    row_table, device_table = tables()
    bf16, f32, i32 = jnp.bfloat16, jnp.float32, jnp.int32
    vmem = pltpu.VMEM
    dma = pltpu.SemaphoreType.DMA
    scratch = [vmem((SRC, 2, QB, BLOCK, PAIR), bf16) for _ in range(HP)] + [
        vmem((2, rows, half_d), bf16),
        vmem(query_weight.shape, bf16),
        vmem(key_weight.shape, bf16),
        vmem(value_weight.shape, bf16),
        vmem(out_weight.shape, bf16),
        vmem(chosen.shape, i32),
        vmem(row_table.shape, f32),
        vmem(device_table.shape, f32),
        vmem((2, ROWS, PAIR), f32),
        vmem((3, width // 256, ROWS, 256), f32),
        vmem((QB, ROWS), f32),
        vmem((ROWS, ROWS), f32),
        vmem((4, CAP * QB, OUT_KEYS), f32),
        vmem((QB, ROWS), i32),
        vmem((SLOTS, CAP * QB, OUT_KEYS), f32),
        vmem((SLOTS, QB, ROWS), i32),
        vmem((HP, SLOTS + 1, ROWS, PAIR), bf16),
        vmem((HP, SLOTS, ROWS, PAIR), bf16),
        vmem((HP, SLOTS, 8, ROWS), f32),
        vmem((HP, SLOTS, ROWS, PAIR), bf16),
        vmem((HP, SLOTS, 8, ROWS), f32),
        vmem((HP, ROWS, PAIR), f32),
        vmem((HP, 8, ROWS), f32),
        vmem((2, HP, ROWS, PAIR), bf16),
        vmem((rows, out_half), bf16),
        vmem((out_half // 256, rows, 256), f32),
        pltpu.SMEM((SLOTS + 1, QB, ROWS), i32),
        dma((8,)),
        dma((10, HP)),
        dma((10, HP)),
        dma((2,)),
        dma((SLOTS, HP)),
        dma((SLOTS, HP)),
        dma((SLOTS, 2)),
        dma((SLOTS, 2)),
        dma((SLOTS, HP)),
        dma((SLOTS, HP)),
        dma((SLOTS, HP)),
        dma((SLOTS, HP)),
        dma((SLOTS + 1,)),
        dma((out_half // 256,)),
    ]
    return pl.pallas_call(
        kernel,
        out_shape=jax.ShapeDtypeStruct((rows, out_half), bf16),
        in_specs=[pl.BlockSpec(memory_space=pl.ANY)] * 8,
        out_specs=pl.BlockSpec(memory_space=pl.ANY),
        scratch_shapes=scratch,
        compiler_params=pltpu.CompilerParams(
            collective_id=0, has_side_effects=True, vmem_limit_bytes=58 * 1024 * 1024
        ),
        name="block_attention",
    )(
        tokens, query_weight, key_weight, value_weight, out_weight, chosen,
        jnp.asarray(row_table), jnp.asarray(device_table),
    )


def solution(mesh):
    placed = (
        P(DP_KV, "tp"),
        P(None, "tp"),
        P(None, "tp"),
        P(None, "tp"),
        P(None, "tp"),
        P(DP_KV, None),
    )
    return jax.shard_map(
        on_device, mesh=mesh, in_specs=placed, out_specs=P(DP_KV, "tp"), check_vma=False
    )
```

```python
import functools

import jax
import jax.numpy as jnp
import numpy as np
from jax import lax
from jax.experimental import pallas as pl
from jax.experimental.pallas import tpu as pltpu
from jax.sharding import PartitionSpec as P

DP_KV = ("dp", "kv")
MESH = pl.DeviceIdType.MESH

HEAD_DIM = 64
BLOCK = 32
CAP = 3
ROWS = 256
QB = 8
XS = 4
ZS = 8
SRC = 8
PAIR = 128
LISTED = CAP * SRC * BLOCK
OUT_KEYS = SRC * BLOCK
HP = 4
SLOTS = 3
MASKED = -1e30
ROTARY_BASE = 500000.0


def tables():
    lane = np.arange(PAIR)
    inverse = ROTARY_BASE ** (-(lane % 32) / 32.0)
    inside = np.arange(ROWS)[:, None] * inverse[None, :]
    device = (np.arange(XS * ZS) * ROWS)[:, None] * inverse[None, :]
    row_table = np.stack([np.cos(inside), np.sin(inside)]).astype(np.float32)
    device_table = np.zeros((XS * ZS, 8, PAIR), np.float32)
    device_table[:, 0] = np.cos(device)
    device_table[:, 1] = np.sin(device)
    return row_table, device_table


def iota(shape, dim):
    return lax.broadcasted_iota(jnp.int32, shape, dim)


def half_scores(q, keys, half):
    q_half = q * half
    return lax.dot_general(
        q_half, keys, (((1,), (1,)), ((), ())), preferred_element_type=jnp.float32
    )


def attend(q, keys, values, bias):
    lane = iota((1, PAIR), 1)
    first = (lane < HEAD_DIM).astype(jnp.float32)
    halves = (first.astype(jnp.bfloat16), (1.0 - first).astype(jnp.bfloat16))
    outs, peaks = [], []
    for half, other in (halves, halves[::-1]):
        scores = half_scores(q, keys, half)
        scores = bias(scores)
        peak = jnp.max(scores, axis=1, keepdims=True)
        weight = jnp.exp(scores - peak).astype(jnp.bfloat16)
        outs.append(
            jnp.dot(weight, values * half + other, preferred_element_type=jnp.float32)
        )
        peaks.append(peak)
    in_first = iota((ROWS, PAIR), 1) < HEAD_DIM
    numerator = jnp.where(in_first, outs[0], outs[1])
    sums = pltpu.roll(jnp.where(in_first, outs[1], outs[0]), HEAD_DIM, 1)
    peak = jnp.where(in_first, peaks[0], peaks[1])
    return numerator, sums, peak


def compact(peak, sums):
    lane = iota((ROWS, PAIR), 1)
    turned = jnp.where(lane % HEAD_DIM < 32, peak, sums).T
    row = iota((8, PAIR), 0)
    packed = jnp.zeros((8, PAIR), jnp.float32)
    for k in range(4):
        part = turned[k * 32 : k * 32 + 8]
        packed = jnp.where(row == 2 * k, part[:, :PAIR], packed)
        packed = jnp.where(row == 2 * k + 1, part[:, PAIR:], packed)
    return packed


def row_of(stats, k):
    return jnp.concatenate([stats[2 * k : 2 * k + 1], stats[2 * k + 1 : 2 * k + 2]], axis=1)


def kernel(
    tok_hbm, wq_hbm, wk_hbm, wv_hbm, ow_hbm, ch_hbm, tab_hbm, dev_hbm, out_hbm, *scratch
):
    kv = scratch[:HP]
    (
        tok, wq, wk, wv, ow, ch, tab, dev, angle, acc, listing, own_bias, pair_bias, table,
        got_bias, got_table, q_buf, o_out, s_out, o_in, s_in, own_o, own_s, att, out_buf, out_acc, small,
        load_sem, send, recv, tok_sem, q_send, q_recv, m_send, m_recv, o_send, o_recv,
        s_send, s_recv, small_sem, out_sem,
    ) = scratch[HP:]
    dp, me, core = (lax.axis_index(a) for a in ("dp", "kv", "tp"))
    z, x = me // XS, me % XS
    pair, odd = z // 2, z % 2
    left, right = (x + XS - 1) % XS, (x + 1) % XS
    other_row = z + 1 - 2 * odd
    half_d = tok.shape[2]
    width = wq.shape[1]

    def at(row, column):
        return (dp, row * XS + column, core)

    mate = (dp, me, 1 - core)

    loads = [
        (tok_hbm, tok.at[core]), (wk_hbm, wk), (wv_hbm, wv), (wq_hbm, wq), (ch_hbm, ch),
        (tab_hbm, tab), (dev_hbm, dev), (ow_hbm, ow),
    ]
    loads = [
        pltpu.make_async_copy(a, b, load_sem.at[i]) for i, (a, b) in enumerate(loads)
    ]
    for i in (0, 1, 2, 3, 5, 6, 4, 7):
        loads[i].start()

    barrier = pltpu.get_barrier_semaphore()

    def greet(device):
        pl.semaphore_signal(barrier, inc=1, device_id=device, device_id_type=MESH)

    greet(mate)
    greet(at(z, left))
    greet(at(z, right))
    for k in range(1, ZS):
        greet(at((z + k) % ZS, x))

    loads[5].wait()
    loads[6].wait()
    dev_cos, dev_sin = dev[me, 0:1, :], dev[me, 1:2, :]
    sign = jnp.where(iota((1, PAIR), 1) % HEAD_DIM < 32, -1.0, 1.0)
    angle[0] = tab[0] * dev_cos - tab[1] * dev_sin
    angle[1] = (tab[1] * dev_cos + tab[0] * dev_sin) * sign

    def remote(src, dst, send_sem, recv_sem, device):
        return pltpu.make_async_remote_copy(
            src_ref=src, dst_ref=dst, send_sem=send_sem, recv_sem=recv_sem,
            device_id=device, device_id_type=MESH,
        )

    loads[0].wait()
    for w, load in ((0, 1), (1, 2), (2, 3)):
        loads[load].wait()
        weight = (wk, wv, wq)[w]
        for c in range(width // 256):
            cols = pl.ds(c * 256, 256)
            acc[w, c] = jnp.dot(
                tok[core], weight[pl.ds(core * half_d, half_d), cols],
                preferred_element_type=jnp.float32,
            )
    pl.semaphore_wait(barrier, 3 + ZS - 1)
    tokens = remote(tok.at[core], tok.at[core], tok_sem.at[0], tok_sem.at[1], mate)
    tokens.start()

    loads[4].wait()
    lane = iota((QB, ROWS), 1)
    lane8 = lane % QB
    chosen = ch[...]
    hit = jnp.zeros((QB, ROWS), jnp.int32)
    for t in range(chosen.shape[1]):
        hit = jnp.where(chosen[:, t : t + 1] == lane, 1, hit)
    need = jnp.max(hit, axis=0, keepdims=True)
    need = jnp.broadcast_to(need, (QB, ROWS))
    need = jnp.where(lane // QB == me, 0, need)
    rank = need
    for k in (1, 2, 4):
        rank = rank + jnp.where(lane8 >= k, pltpu.roll(rank, k, 1), 0)
    rank = rank - need
    sub = iota((QB, ROWS), 0)
    listed = jnp.zeros((QB, ROWS), jnp.int32)
    placed = []
    for slot in range(CAP):
        here = jnp.where(rank == slot, need, 0)
        placed.append((hit * here).astype(jnp.float32))
        where = here * lane8
        for k in (1, 2, 4):
            where = where + jnp.where(lane8 >= k, pltpu.roll(where, k, 1), 0)
        listed = jnp.where(sub == slot, where, listed)
    table[...] = listed
    placed = jnp.concatenate(placed, axis=0).astype(jnp.bfloat16)
    for k in range(4):
        spread = (iota((ROWS, OUT_KEYS), 0) // QB) == (iota((ROWS, OUT_KEYS), 1) // BLOCK + k * SRC)
        spread = spread.astype(jnp.float32).astype(jnp.bfloat16)
        found = jnp.dot(placed, spread, preferred_element_type=jnp.float32)
        pair_bias[k] = ((found - 1.0) * -MASKED).astype(jnp.bfloat16)
    spread = iota((ROWS, ROWS), 0) == (iota((ROWS, ROWS), 1) // BLOCK + me * QB)
    spread = spread.astype(jnp.float32).astype(jnp.bfloat16)
    found = jnp.dot(
        hit.astype(jnp.float32).astype(jnp.bfloat16), spread, preferred_element_type=jnp.float32
    )
    listing[...] = (found - 1.0) * -MASKED
    for b in range(QB):
        rows = pl.ds(b * BLOCK, BLOCK)
        causal = iota((BLOCK, ROWS), 1) <= iota((BLOCK, ROWS), 0) + b * BLOCK
        own_bias[rows, :] = jnp.where(causal, listing[b : b + 1, :], MASKED)

    for k in range(SLOTS):
        @pl.when(pair <= k)
        def _():
            for hp in range(HP):
                o_in[hp, k] = jnp.zeros((ROWS, PAIR), jnp.bfloat16)
                s_in[hp, k] = jnp.full((8, PAIR), MASKED, jnp.float32)

    theirs = remote(tok.at[1 - core], tok.at[1 - core], tok_sem.at[0], tok_sem.at[1], mate)
    theirs.wait_recv()

    def project(w, c):
        weight = (wk, wv, wq)[w]
        cols = pl.ds(c * 256, 256)
        return acc[w, c] + jnp.dot(
            tok[1 - core], weight[pl.ds((1 - core) * half_d, half_d), cols],
            preferred_element_type=jnp.float32,
        )

    low = iota((ROWS, PAIR), 1) % HEAD_DIM < 32

    def turn(part):
        partner = jnp.where(low, pltpu.roll(part, PAIR - 32, 1), pltpu.roll(part, 32, 1))
        return part * angle[0] + partner * angle[1]

    def blocked(part):
        return part.astype(jnp.bfloat16).reshape(QB, BLOCK, PAIR)

    own = odd * XS + x
    mated = (1 - odd) * XS + x
    far = (x + 2) % XS

    def hop(kind, hp, source, device, which=None):
        part = kv[hp].at[source] if which is None else kv[hp].at[source, which]
        return remote(part, part, send.at[kind, hp], recv.at[kind, hp], device)

    def send_own(hp):
        hop(1, hp, own, at(z, right)).start()
        hop(2, hp, own, at(z, left)).start()

    def send_across(hp):
        hop(0, hp, own, at(other_row, x)).start()

    turn_back = (z - 3) // 2 - 1
    q_row = [1 - z // 5, 3 - turn_back * turn_back, z * 0 + 5]
    q_slot = [(z + 1) % 3, (z // 2) % 2, z % 2]

    def q_copy(k, hp, slot):
        return remote(
            q_buf.at[hp, SLOTS], q_buf.at[hp, slot], q_send.at[k, hp], q_recv.at[slot, hp],
            at(q_row[k], x),
        )

    def meta_copies(k, slot):
        return (
            remote(pair_bias.at[k], got_bias.at[slot], m_send.at[k, 0], m_recv.at[slot, 0],
                   at(q_row[k], x)),
            remote(table, got_table.at[slot], m_send.at[k, 1], m_recv.at[slot, 1],
                   at(q_row[k], x)),
        )

    def send_queries(hp):
        for k in range(SLOTS):
            @pl.when(pair > k)
            def _():
                if hp == 0:
                    for copy in meta_copies(k, q_slot[k]):
                        copy.start()
                q_copy(k, hp, q_slot[k]).start()

    for c in range(width // 256):
        keys, values = project(0, c), project(1, c)
        for i in range(2):
            hp = 2 * c + i
            part = slice(i * PAIR, (i + 1) * PAIR)
            kv[hp][own, 0] = blocked(turn(keys[:, part]))
            kv[hp][own, 1] = blocked(values[:, part])
            if hp == 0:
                send_across(hp)
            if c == 0:
                send_own(hp)
        queries = project(2, c)
        for i in range(2):
            hp = 2 * c + i
            part = slice(i * PAIR, (i + 1) * PAIR)
            turned = turn(queries[:, part]).astype(jnp.bfloat16).astype(jnp.float32)
            q_buf[hp, SLOTS] = (turned * HEAD_DIM**-0.5).astype(jnp.bfloat16)
            if hp == 0:
                send_queries(0)
                send_across(1)

    own_small = pltpu.make_async_copy(table, small.at[SLOTS], small_sem.at[SLOTS])
    own_small.start()

    own_left, own_right, own_far = odd * XS + left, odd * XS + right, odd * XS + far
    row2 = (1 - odd) * XS
    mate_left, mate_right, mate_far = row2 + left, row2 + right, row2 + far

    def pass_mate(hp):
        hop(0, hp, mated, at(other_row, x)).wait_recv()
        hop(3, hp, mated, at(z, right)).start()
        hop(4, hp, mated, at(z, left)).start()

    def relay_own(hp):
        hop(1, hp, own_left, at(z, right)).wait_recv()
        hop(5, hp, own_left, at(z, right), 0).start()
        hop(2, hp, own_right, at(z, left)).wait_recv()
        hop(6, hp, own_right, at(z, left), 1).start()

    def relay_mate(hp):
        hop(3, hp, mate_left, at(z, right)).wait_recv()
        hop(7, hp, mate_left, at(z, right), 0).start()
        hop(4, hp, mate_right, at(z, left)).wait_recv()
        hop(8, hp, mate_right, at(z, left), 1).start()

    def complete(hp):
        hop(5, hp, own_far, at(z, right), 0).wait_recv()
        hop(6, hp, own_far, at(z, left), 1).wait_recv()
        hop(7, hp, mate_far, at(z, right), 0).wait_recv()
        hop(8, hp, mate_far, at(z, left), 1).wait_recv()

    def gathered(hp, slot, which):
        blocks = []
        for k in range(CAP):
            for s in range(SRC):
                index = small[slot, k, pair * (QB * SRC) + s * QB + QB - 1]
                blocks.append(kv[hp][s, which, index])
        return blocks

    def wide_bias(bias):
        return jnp.concatenate([bias[k * QB : (k + 1) * QB] for k in range(CAP)], axis=1)

    pair3 = pair // 3
    pair2, pair1, pair0 = (pair // 2) * (1 - pair3), (pair % 2) * (1 - pair3), (3 - pair) // 3
    base = pair0 * (5 - 3 * odd) + pair1 * (4 + odd) + pair2 * (8 - 2 * odd) + pair3 * 8

    def sender(slot):
        return base + slot * (1 + 2 * pair1 * (1 - odd)) + (slot // 2) * 5 * pair1 * odd


    def partial_copies(hp, slot, k):
        row = sender(slot)
        return (
            remote(o_out.at[hp, slot], o_in.at[hp, k], o_send.at[slot, hp], o_recv.at[k, hp],
                   at(row, x)),
            remote(s_out.at[hp, slot], s_in.at[hp, k], s_send.at[slot, hp], s_recv.at[k, hp],
                   at(row, x)),
        )

    def visitors(hp):
        @pl.loop(0, SLOTS)
        def _(slot):
            @pl.when(slot == SLOTS - 1)
            def _():
                keep_ring_going(hp)

            @pl.when(sender(slot) < ZS)
            def _():
                if hp == 0:
                    for ref, i in ((got_bias, 0), (got_table, 1)):
                        remote(ref.at[slot], ref.at[slot], m_send.at[0, i], m_recv.at[slot, i],
                               mate).wait_recv()
                    copy = pltpu.make_async_copy(
                        got_table.at[slot], small.at[slot], small_sem.at[slot]
                    )
                    copy.start()
                    copy.wait()
                q_ref = q_buf.at[hp, slot]
                remote(q_ref, q_ref, q_send.at[0, hp], q_recv.at[slot, hp], mate).wait_recv()
                keys = jnp.concatenate(gathered(hp, slot, 0), axis=0)
                values = jnp.concatenate(gathered(hp, slot, 1), axis=0)
                bias = wide_bias(got_bias[slot].astype(jnp.float32))

                def masked(scores):
                    scores = scores.reshape(QB, BLOCK, LISTED) + bias[:, None, :]
                    return scores.reshape(ROWS, LISTED)

                numerator, sums, peak = attend(q_ref[...], keys, values, masked)
                o_out[hp, slot] = (numerator / sums).astype(jnp.bfloat16)
                s_out[hp, slot] = compact(peak, sums)
                for copy in partial_copies(hp, slot, pair):
                    copy.start()

    def own_queries(hp):
        if hp == 0:
            own_small.wait()
        keys = jnp.concatenate(gathered(hp, SLOTS, 0) + [kv[hp][own, 0].reshape(ROWS, PAIR)], axis=0)
        values = jnp.concatenate(gathered(hp, SLOTS, 1) + [kv[hp][own, 1].reshape(ROWS, PAIR)], axis=0)
        bias = wide_bias(pair_bias[pair].astype(jnp.float32))

        def masked(scores):
            others = scores[:, :LISTED].reshape(QB, BLOCK, LISTED) + bias[:, None, :]
            mine = scores[:, LISTED:] + own_bias[...]
            return jnp.concatenate([others.reshape(ROWS, LISTED), mine], axis=1)

        numerator, sums, peak = attend(q_buf[hp, SLOTS], keys, values, masked)
        own_o[hp] = numerator / sums
        own_s[hp] = compact(peak, sums)

    def att_copy(hp, side):
        part = att.at[side, hp]
        return remote(part, part, send.at[9, hp], recv.at[9, hp], mate)

    def merge(hp):
        for k in range(SLOTS):
            @pl.when(pair > k)
            def _():
                for ref, sem in ((o_in, o_recv), (s_in, s_recv)):
                    part = ref.at[hp, k]
                    remote(part, part, o_send.at[0, hp], sem.at[k, hp], mate).wait_recv()
        stats = [own_s[hp]] + [s_in[hp, k] for k in range(SLOTS)]
        shares = [[None, None] for _ in stats]
        for h in range(2):
            peaks = [row_of(s, 2 * h) for s in stats]
            top = functools.reduce(jnp.maximum, peaks)
            weights = [
                row_of(s, 2 * h + 1) * jnp.exp(p - top) for s, p in zip(stats, peaks)
            ]
            scale = 1.0 / functools.reduce(jnp.add, weights)
            for i, w in enumerate(weights):
                shares[i][h] = w * scale
        rows = [jnp.broadcast_to(s, (16, ROWS)) for share in shares for s in share]
        turned = jnp.concatenate(rows, axis=0).T
        in_first = iota((ROWS, PAIR), 1) < HEAD_DIM
        total = jnp.zeros((ROWS, PAIR), jnp.float32)
        for i in range(1 + SLOTS):
            share = jnp.where(
                in_first, turned[:, i * 32 : i * 32 + 1], turned[:, i * 32 + 16 : i * 32 + 17]
            )
            part = own_o[hp] if i == 0 else o_in[hp, i - 1].astype(jnp.float32)
            total = total + share * part
        att[core, hp] = total.astype(jnp.bfloat16)
        att_copy(hp, core).start()

    def project_out(hp):
        att_copy(hp, 1 - core).wait_recv()
        if hp == 0:
            loads[7].wait()
        heads = jnp.concatenate([att[s, hp] for s in range(2)], axis=1)
        outs = []
        for c in range(ow.shape[1] // 256):
            cols = pl.ds(c * 256, 256)
            weight = jnp.concatenate(
                [ow[pl.ds(s * width + hp * PAIR, PAIR), cols] for s in range(2)], axis=0
            )
            out = jnp.dot(heads, weight, preferred_element_type=jnp.float32)
            if hp:
                out = out + out_acc[c]
            if hp < HP - 1:
                out_acc[c] = out
            outs.append(out)
        return outs

    pass_mate(0)
    send_queries(1)
    relay_own(0)
    send_own(2)
    relay_mate(0)
    pass_mate(1)
    relay_own(1)
    send_own(3)
    send_across(2)
    send_queries(2)

    def keep_ring_going(hp):
        if hp + 1 < HP:
            relay_mate(hp + 1)
        if hp + 2 < HP:
            pass_mate(hp + 2)
            relay_own(hp + 2)
        if hp == 0:
            send_across(3)
            send_queries(3)

    for hp in range(HP):
        complete(hp)
        visitors(hp)
        own_queries(hp)
        if hp :
            merge(hp - 1)
        if hp > 1:
            project_out(hp - 2)
    merge(HP - 1)
    project_out(HP - 2)

    stores = []
    for c, out in enumerate(project_out(HP - 1)):
        cols = pl.ds(c * 256, 256)
        out_buf[:, cols] = out.astype(jnp.bfloat16)
        store = pltpu.make_async_copy(
            out_buf.at[:, cols], out_hbm.at[:, cols], out_sem.at[c]
        )
        store.start()
        stores.append(store)

    tokens.wait_send()
    for hp in range(HP):
        hop(0, hp, own, at(other_row, x)).wait_send()
        hop(1, hp, own, at(z, right)).wait_send()
        hop(2, hp, own, at(z, left)).wait_send()
        hop(3, hp, mated, at(z, right)).wait_send()
        hop(4, hp, mated, at(z, left)).wait_send()
        hop(5, hp, own_left, at(z, right), 0).wait_send()
        hop(6, hp, own_right, at(z, left), 1).wait_send()
        hop(7, hp, mate_left, at(z, right), 0).wait_send()
        hop(8, hp, mate_right, at(z, left), 1).wait_send()
        att_copy(hp, core).wait_send()
    for k in range(SLOTS):
        @pl.when(pair > k)
        def _():
            for copy in meta_copies(k, q_slot[k]):
                copy.wait_send()
            for hp in range(HP):
                q_copy(k, hp, q_slot[k]).wait_send()

    @pl.loop(0, SLOTS)
    def _(slot):
        @pl.when(sender(slot) < ZS)
        def _():
            for hp in range(HP):
                for copy in partial_copies(hp, slot, pair):
                    copy.wait_send()

    for store in stores:
        store.wait()


def on_device(tokens, query_weight, key_weight, value_weight, out_weight, chosen):
    rows, half_d = tokens.shape
    width = query_weight.shape[1]
    out_half = out_weight.shape[1]
    row_table, device_table = tables()
    bf16, f32, i32 = jnp.bfloat16, jnp.float32, jnp.int32
    vmem = pltpu.VMEM
    dma = pltpu.SemaphoreType.DMA
    scratch = [vmem((SRC, 2, QB, BLOCK, PAIR), bf16) for _ in range(HP)] + [
        vmem((2, rows, half_d), bf16),
        vmem(query_weight.shape, bf16),
        vmem(key_weight.shape, bf16),
        vmem(value_weight.shape, bf16),
        vmem(out_weight.shape, bf16),
        vmem(chosen.shape, i32),
        vmem(row_table.shape, f32),
        vmem(device_table.shape, f32),
        vmem((2, ROWS, PAIR), f32),
        vmem((3, width // 256, ROWS, 256), f32),
        vmem((QB, ROWS), f32),
        vmem((ROWS, ROWS), f32),
        vmem((4, CAP * QB, OUT_KEYS), bf16),
        vmem((QB, ROWS), i32),
        vmem((SLOTS, CAP * QB, OUT_KEYS), bf16),
        vmem((SLOTS, QB, ROWS), i32),
        vmem((HP, SLOTS + 1, ROWS, PAIR), bf16),
        vmem((HP, SLOTS, ROWS, PAIR), bf16),
        vmem((HP, SLOTS, 8, PAIR), f32),
        vmem((HP, SLOTS, ROWS, PAIR), bf16),
        vmem((HP, SLOTS, 8, PAIR), f32),
        vmem((HP, ROWS, PAIR), f32),
        vmem((HP, 8, PAIR), f32),
        vmem((2, HP, ROWS, PAIR), bf16),
        vmem((rows, out_half), bf16),
        vmem((out_half // 256, rows, 256), f32),
        pltpu.SMEM((SLOTS + 1, QB, ROWS), i32),
        dma((8,)),
        dma((10, HP)),
        dma((10, HP)),
        dma((2,)),
        dma((SLOTS, HP)),
        dma((SLOTS, HP)),
        dma((SLOTS, 2)),
        dma((SLOTS, 2)),
        dma((SLOTS, HP)),
        dma((SLOTS, HP)),
        dma((SLOTS, HP)),
        dma((SLOTS, HP)),
        dma((SLOTS + 1,)),
        dma((out_half // 256,)),
    ]
    return pl.pallas_call(
        kernel,
        out_shape=jax.ShapeDtypeStruct((rows, out_half), bf16),
        in_specs=[pl.BlockSpec(memory_space=pl.ANY)] * 8,
        out_specs=pl.BlockSpec(memory_space=pl.ANY),
        scratch_shapes=scratch,
        compiler_params=pltpu.CompilerParams(
            collective_id=0, has_side_effects=True, vmem_limit_bytes=58 * 1024 * 1024
        ),
        name="block_attention",
    )(
        tokens, query_weight, key_weight, value_weight, out_weight, chosen,
        jnp.asarray(row_table), jnp.asarray(device_table),
    )


def solution(mesh):
    placed = (
        P(DP_KV, "tp"),
        P(None, "tp"),
        P(None, "tp"),
        P(None, "tp"),
        P(None, "tp"),
        P(DP_KV, None),
    )
    return jax.shard_map(
        on_device, mesh=mesh, in_specs=placed, out_specs=P(DP_KV, "tp"), check_vma=False
    )
```

```python
import functools

import jax
import jax.numpy as jnp
import numpy as np
from jax import lax
from jax.experimental import pallas as pl
from jax.experimental.pallas import tpu as pltpu
from jax.sharding import PartitionSpec as P

DP_KV = ("dp", "kv")
MESH = pl.DeviceIdType.MESH

HEAD_DIM = 64
BLOCK = 32
CAP = 3
ROWS = 256
QB = 8
XS = 4
ZS = 8
SRC = 8
PAIR = 128
LISTED = CAP * SRC * BLOCK
OUT_KEYS = SRC * BLOCK
HP = 4
SLOTS = 3
MASKED = -1e30
ROTARY_BASE = 500000.0


def tables():
    lane = np.arange(PAIR)
    inverse = ROTARY_BASE ** (-(lane % 32) / 32.0)
    inside = np.arange(ROWS)[:, None] * inverse[None, :]
    device = (np.arange(XS * ZS) * ROWS)[:, None] * inverse[None, :]
    row_table = np.stack([np.cos(inside), np.sin(inside)]).astype(np.float32)
    device_table = np.zeros((XS * ZS, 8, PAIR), np.float32)
    device_table[:, 0] = np.cos(device)
    device_table[:, 1] = np.sin(device)
    return row_table, device_table


def iota(shape, dim):
    return lax.broadcasted_iota(jnp.int32, shape, dim)


def half_scores(q, keys, half):
    q_half = q * half
    return lax.dot_general(
        q_half, keys, (((1,), (1,)), ((), ())), preferred_element_type=jnp.float32
    )


def attend(q, keys, values, bias):
    lane = iota((1, PAIR), 1)
    first = (lane < HEAD_DIM).astype(jnp.float32)
    halves = (first.astype(jnp.bfloat16), (1.0 - first).astype(jnp.bfloat16))
    outs, peaks = [], []
    for half, other in (halves, halves[::-1]):
        scores = half_scores(q, keys, half)
        scores = bias(scores)
        peak = jnp.max(scores, axis=1, keepdims=True)
        weight = jnp.exp(scores - peak).astype(jnp.bfloat16)
        outs.append(
            jnp.dot(weight, values * half + other, preferred_element_type=jnp.float32)
        )
        peaks.append(peak)
    in_first = iota((ROWS, PAIR), 1) < HEAD_DIM
    numerator = jnp.where(in_first, outs[0], outs[1])
    sums = pltpu.roll(jnp.where(in_first, outs[1], outs[0]), HEAD_DIM, 1)
    peak = jnp.where(in_first, peaks[0], peaks[1])
    return numerator, sums, peak


def compact(peak, sums):
    lane = iota((ROWS, PAIR), 1)
    turned = jnp.where(lane % HEAD_DIM < 32, peak, sums).T
    row = iota((8, PAIR), 0)
    packed = jnp.zeros((8, PAIR), jnp.float32)
    for k in range(4):
        part = turned[k * 32 : k * 32 + 8]
        packed = jnp.where(row == 2 * k, part[:, :PAIR], packed)
        packed = jnp.where(row == 2 * k + 1, part[:, PAIR:], packed)
    return packed


def row_of(stats, k):
    return jnp.concatenate([stats[2 * k : 2 * k + 1], stats[2 * k + 1 : 2 * k + 2]], axis=1)


def kernel(
    tok_hbm, wq_hbm, wk_hbm, wv_hbm, ow_hbm, ch_hbm, tab_hbm, dev_hbm, out_hbm, *scratch
):
    kv = scratch[:HP]
    (
        tok, wq, wk, wv, ow, ch, tab, dev, angle, acc, listing, own_bias, pair_bias, table,
        got_bias, got_table, q_buf, o_out, s_out, o_in, s_in, own_o, own_s, att, out_buf, out_acc, small,
        load_sem, send, recv, tok_sem, q_send, q_recv, m_send, m_recv, o_send, o_recv,
        s_send, s_recv, small_sem, out_sem,
    ) = scratch[HP:]
    dp, me, core = (lax.axis_index(a) for a in ("dp", "kv", "tp"))
    z, x = me // XS, me % XS
    pair, odd = z // 2, z % 2
    left, right = (x + XS - 1) % XS, (x + 1) % XS
    other_row = z + 1 - 2 * odd
    half_d = tok.shape[2]
    width = wq.shape[1]

    def at(row, column):
        return (dp, row * XS + column, core)

    mate = (dp, me, 1 - core)

    loads = [
        (tok_hbm, tok.at[core]), (wk_hbm, wk), (wv_hbm, wv), (wq_hbm, wq), (ch_hbm, ch),
        (tab_hbm, tab), (dev_hbm, dev), (ow_hbm, ow),
    ]
    loads = [
        pltpu.make_async_copy(a, b, load_sem.at[i]) for i, (a, b) in enumerate(loads)
    ]
    for i in (0, 1, 2, 3, 5, 6, 4, 7):
        loads[i].start()

    barrier = pltpu.get_barrier_semaphore()

    def greet(device):
        pl.semaphore_signal(barrier, inc=1, device_id=device, device_id_type=MESH)

    greet(mate)
    greet(at(z, left))
    greet(at(z, right))
    for k in range(1, ZS):
        if k != ZS // 2:
            greet(at((z + k) % ZS, x))

    loads[5].wait()
    loads[6].wait()
    dev_cos, dev_sin = dev[me, 0:1, :], dev[me, 1:2, :]
    sign = jnp.where(iota((1, PAIR), 1) % HEAD_DIM < 32, -1.0, 1.0)
    angle[0] = tab[0] * dev_cos - tab[1] * dev_sin
    angle[1] = (tab[1] * dev_cos + tab[0] * dev_sin) * sign

    def remote(src, dst, send_sem, recv_sem, device):
        return pltpu.make_async_remote_copy(
            src_ref=src, dst_ref=dst, send_sem=send_sem, recv_sem=recv_sem,
            device_id=device, device_id_type=MESH,
        )

    loads[0].wait()
    for w, load in ((0, 1), (1, 2), (2, 3)):
        loads[load].wait()
        weight = (wk, wv, wq)[w]
        for c in range(width // 256):
            cols = pl.ds(c * 256, 256)
            acc[w, c] = jnp.dot(
                tok[core], weight[pl.ds(core * half_d, half_d), cols],
                preferred_element_type=jnp.float32,
            )
    pl.semaphore_wait(barrier, 3 + ZS - 2)
    tokens = remote(tok.at[core], tok.at[core], tok_sem.at[0], tok_sem.at[1], mate)
    tokens.start()

    loads[4].wait()
    lane = iota((QB, ROWS), 1)
    lane8 = lane % QB
    chosen = ch[...]
    hit = jnp.zeros((QB, ROWS), jnp.int32)
    for t in range(chosen.shape[1]):
        hit = jnp.where(chosen[:, t : t + 1] == lane, 1, hit)
    need = jnp.max(hit, axis=0, keepdims=True)
    need = jnp.broadcast_to(need, (QB, ROWS))
    need = jnp.where(lane // QB == me, 0, need)
    rank = need
    for k in (1, 2, 4):
        rank = rank + jnp.where(lane8 >= k, pltpu.roll(rank, k, 1), 0)
    rank = rank - need
    sub = iota((QB, ROWS), 0)
    listed = jnp.zeros((QB, ROWS), jnp.int32)
    placed = []
    for slot in range(CAP):
        here = jnp.where(rank == slot, need, 0)
        placed.append((hit * here).astype(jnp.float32))
        where = here * lane8
        for k in (1, 2, 4):
            where = where + jnp.where(lane8 >= k, pltpu.roll(where, k, 1), 0)
        listed = jnp.where(sub == slot, where, listed)
    table[...] = listed
    placed = jnp.concatenate(placed, axis=0).astype(jnp.bfloat16)
    for k in range(4):
        spread = (iota((ROWS, OUT_KEYS), 0) // QB) == (iota((ROWS, OUT_KEYS), 1) // BLOCK + k * SRC)
        spread = spread.astype(jnp.float32).astype(jnp.bfloat16)
        found = jnp.dot(placed, spread, preferred_element_type=jnp.float32)
        pair_bias[k] = ((found - 1.0) * -MASKED).astype(jnp.bfloat16)
    spread = iota((ROWS, ROWS), 0) == (iota((ROWS, ROWS), 1) // BLOCK + me * QB)
    spread = spread.astype(jnp.float32).astype(jnp.bfloat16)
    found = jnp.dot(
        hit.astype(jnp.float32).astype(jnp.bfloat16), spread, preferred_element_type=jnp.float32
    )
    listing[...] = (found - 1.0) * -MASKED
    for b in range(QB):
        rows = pl.ds(b * BLOCK, BLOCK)
        causal = iota((BLOCK, ROWS), 1) <= iota((BLOCK, ROWS), 0) + b * BLOCK
        own_bias[rows, :] = jnp.where(causal, listing[b : b + 1, :], MASKED)

    for k in range(SLOTS):
        @pl.when(pair <= k)
        def _():
            for hp in range(HP):
                o_in[hp, k] = jnp.zeros((ROWS, PAIR), jnp.bfloat16)
                s_in[hp, k] = jnp.full((8, PAIR), MASKED, jnp.float32)

    theirs = remote(tok.at[1 - core], tok.at[1 - core], tok_sem.at[0], tok_sem.at[1], mate)
    theirs.wait_recv()

    def project(w, c):
        weight = (wk, wv, wq)[w]
        cols = pl.ds(c * 256, 256)
        return acc[w, c] + jnp.dot(
            tok[1 - core], weight[pl.ds((1 - core) * half_d, half_d), cols],
            preferred_element_type=jnp.float32,
        )

    low = iota((ROWS, PAIR), 1) % HEAD_DIM < 32

    def turn(part):
        partner = jnp.where(low, pltpu.roll(part, PAIR - 32, 1), pltpu.roll(part, 32, 1))
        return part * angle[0] + partner * angle[1]

    def blocked(part):
        return part.astype(jnp.bfloat16).reshape(QB, BLOCK, PAIR)

    own = odd * XS + x
    mated = (1 - odd) * XS + x
    far = (x + 2) % XS

    def hop(kind, hp, source, device, which=None):
        part = kv[hp].at[source] if which is None else kv[hp].at[source, which]
        return remote(part, part, send.at[kind, hp], recv.at[kind, hp], device)

    def send_own(hp):
        hop(1, hp, own, at(z, right)).start()
        hop(2, hp, own, at(z, left)).start()

    def send_across(hp):
        hop(0, hp, own, at(other_row, x)).start()

    turn_back = (z - 3) // 2 - 1
    q_row = [1 - z // 5, 3 - turn_back * turn_back, z * 0 + 5]
    q_slot = [(z + 1) % 3, (z // 2) % 2, z % 2]

    def q_copy(k, hp, slot):
        return remote(
            q_buf.at[hp, SLOTS], q_buf.at[hp, slot], q_send.at[k, hp], q_recv.at[slot, hp],
            at(q_row[k], x),
        )

    def meta_copies(k, slot):
        return (
            remote(pair_bias.at[k], got_bias.at[slot], m_send.at[k, 0], m_recv.at[slot, 0],
                   at(q_row[k], x)),
            remote(table, got_table.at[slot], m_send.at[k, 1], m_recv.at[slot, 1],
                   at(q_row[k], x)),
        )

    def send_queries(hp):
        for k in range(SLOTS):
            @pl.when(pair > k)
            def _():
                if hp == 0:
                    for copy in meta_copies(k, q_slot[k]):
                        copy.start()
                q_copy(k, hp, q_slot[k]).start()

    for c in range(width // 256):
        keys, values = project(0, c), project(1, c)
        for i in range(2):
            hp = 2 * c + i
            part = slice(i * PAIR, (i + 1) * PAIR)
            kv[hp][own, 0] = blocked(turn(keys[:, part]))
            kv[hp][own, 1] = blocked(values[:, part])
            if hp == 0:
                send_across(hp)
            if c == 0:
                send_own(hp)
        queries = project(2, c)
        for i in range(2):
            hp = 2 * c + i
            part = slice(i * PAIR, (i + 1) * PAIR)
            turned = turn(queries[:, part]).astype(jnp.bfloat16).astype(jnp.float32)
            q_buf[hp, SLOTS] = (turned * HEAD_DIM**-0.5).astype(jnp.bfloat16)
            if hp == 0:
                send_queries(0)
                send_across(1)

    own_small = pltpu.make_async_copy(table, small.at[SLOTS], small_sem.at[SLOTS])
    own_small.start()

    own_left, own_right, own_far = odd * XS + left, odd * XS + right, odd * XS + far
    row2 = (1 - odd) * XS
    mate_left, mate_right, mate_far = row2 + left, row2 + right, row2 + far

    def pass_mate(hp):
        hop(0, hp, mated, at(other_row, x)).wait_recv()
        hop(3, hp, mated, at(z, right)).start()
        hop(4, hp, mated, at(z, left)).start()

    def relay_own(hp):
        hop(1, hp, own_left, at(z, right)).wait_recv()
        hop(5, hp, own_left, at(z, right), 0).start()
        hop(2, hp, own_right, at(z, left)).wait_recv()
        hop(6, hp, own_right, at(z, left), 1).start()

    def relay_mate(hp):
        hop(3, hp, mate_left, at(z, right)).wait_recv()
        hop(7, hp, mate_left, at(z, right), 0).start()
        hop(4, hp, mate_right, at(z, left)).wait_recv()
        hop(8, hp, mate_right, at(z, left), 1).start()

    def complete(hp):
        hop(5, hp, own_far, at(z, right), 0).wait_recv()
        hop(6, hp, own_far, at(z, left), 1).wait_recv()
        hop(7, hp, mate_far, at(z, right), 0).wait_recv()
        hop(8, hp, mate_far, at(z, left), 1).wait_recv()

    def gathered(hp, slot, which):
        blocks = []
        for k in range(CAP):
            for s in range(SRC):
                index = small[slot, k, pair * (QB * SRC) + s * QB + QB - 1]
                blocks.append(kv[hp][s, which, index])
        return blocks

    def wide_bias(bias):
        return jnp.concatenate([bias[k * QB : (k + 1) * QB] for k in range(CAP)], axis=1)

    pair3 = pair // 3
    pair2, pair1, pair0 = (pair // 2) * (1 - pair3), (pair % 2) * (1 - pair3), (3 - pair) // 3
    base = pair0 * (5 - 3 * odd) + pair1 * (4 + odd) + pair2 * (8 - 2 * odd) + pair3 * 8

    def sender(slot):
        return base + slot * (1 + 2 * pair1 * (1 - odd)) + (slot // 2) * 5 * pair1 * odd


    def partial_copies(hp, slot, k):
        row = sender(slot)
        return (
            remote(o_out.at[hp, slot], o_in.at[hp, k], o_send.at[slot, hp], o_recv.at[k, hp],
                   at(row, x)),
            remote(s_out.at[hp, slot], s_in.at[hp, k], s_send.at[slot, hp], s_recv.at[k, hp],
                   at(row, x)),
        )

    def visitors(hp):
        @pl.loop(0, SLOTS)
        def _(slot):
            @pl.when(slot == SLOTS - 1)
            def _():
                keep_ring_going(hp)

            @pl.when(sender(slot) < ZS)
            def _():
                if hp == 0:
                    for ref, i in ((got_bias, 0), (got_table, 1)):
                        remote(ref.at[slot], ref.at[slot], m_send.at[0, i], m_recv.at[slot, i],
                               mate).wait_recv()
                    copy = pltpu.make_async_copy(
                        got_table.at[slot], small.at[slot], small_sem.at[slot]
                    )
                    copy.start()
                    copy.wait()
                q_ref = q_buf.at[hp, slot]
                remote(q_ref, q_ref, q_send.at[0, hp], q_recv.at[slot, hp], mate).wait_recv()
                keys = jnp.concatenate(gathered(hp, slot, 0), axis=0)
                values = jnp.concatenate(gathered(hp, slot, 1), axis=0)
                bias = wide_bias(got_bias[slot].astype(jnp.float32))

                def masked(scores):
                    scores = scores.reshape(QB, BLOCK, LISTED) + bias[:, None, :]
                    return scores.reshape(ROWS, LISTED)

                numerator, sums, peak = attend(q_ref[...], keys, values, masked)
                o_out[hp, slot] = (numerator / sums).astype(jnp.bfloat16)
                s_out[hp, slot] = compact(peak, sums)
                for copy in partial_copies(hp, slot, pair):
                    copy.start()

    def own_queries(hp):
        if hp == 0:
            own_small.wait()
        keys = jnp.concatenate(gathered(hp, SLOTS, 0) + [kv[hp][own, 0].reshape(ROWS, PAIR)], axis=0)
        values = jnp.concatenate(gathered(hp, SLOTS, 1) + [kv[hp][own, 1].reshape(ROWS, PAIR)], axis=0)
        bias = wide_bias(pair_bias[pair].astype(jnp.float32))

        def masked(scores):
            others = scores[:, :LISTED].reshape(QB, BLOCK, LISTED) + bias[:, None, :]
            mine = scores[:, LISTED:] + own_bias[...]
            return jnp.concatenate([others.reshape(ROWS, LISTED), mine], axis=1)

        numerator, sums, peak = attend(q_buf[hp, SLOTS], keys, values, masked)
        own_o[hp] = numerator / sums
        own_s[hp] = compact(peak, sums)

    def att_copy(hp, side):
        part = att.at[side, hp]
        return remote(part, part, send.at[9, hp], recv.at[9, hp], mate)

    def merge(hp):
        for k in range(SLOTS):
            @pl.when(pair > k)
            def _():
                for ref, sem in ((o_in, o_recv), (s_in, s_recv)):
                    part = ref.at[hp, k]
                    remote(part, part, o_send.at[0, hp], sem.at[k, hp], mate).wait_recv()
        stats = [own_s[hp]] + [s_in[hp, k] for k in range(SLOTS)]
        shares = [[None, None] for _ in stats]
        for h in range(2):
            peaks = [row_of(s, 2 * h) for s in stats]
            top = functools.reduce(jnp.maximum, peaks)
            weights = [
                row_of(s, 2 * h + 1) * jnp.exp(p - top) for s, p in zip(stats, peaks)
            ]
            scale = 1.0 / functools.reduce(jnp.add, weights)
            for i, w in enumerate(weights):
                shares[i][h] = w * scale
        rows = [jnp.broadcast_to(s, (16, ROWS)) for share in shares for s in share]
        turned = jnp.concatenate(rows, axis=0).T
        in_first = iota((ROWS, PAIR), 1) < HEAD_DIM
        total = jnp.zeros((ROWS, PAIR), jnp.float32)
        for i in range(1 + SLOTS):
            share = jnp.where(
                in_first, turned[:, i * 32 : i * 32 + 1], turned[:, i * 32 + 16 : i * 32 + 17]
            )
            part = own_o[hp] if i == 0 else o_in[hp, i - 1].astype(jnp.float32)
            total = total + share * part
        att[core, hp] = total.astype(jnp.bfloat16)
        att_copy(hp, core).start()

    def out_copy(c):
        cols = pl.ds(c * 256, 256)
        return pltpu.make_async_copy(out_buf.at[:, cols], out_hbm.at[:, cols], out_sem.at[c])

    def project_out(hp):
        att_copy(hp, 1 - core).wait_recv()
        if hp == 0:
            loads[7].wait()
        heads = jnp.concatenate([att[s, hp] for s in range(2)], axis=1)
        for c in range(ow.shape[1] // 256):
            cols = pl.ds(c * 256, 256)
            weight = jnp.concatenate(
                [ow[pl.ds(s * width + hp * PAIR, PAIR), cols] for s in range(2)], axis=0
            )
            out = jnp.dot(heads, weight, preferred_element_type=jnp.float32)
            if hp:
                out = out + out_acc[c]
            if hp < HP - 1:
                out_acc[c] = out
            else:
                out_buf[:, cols] = out.astype(jnp.bfloat16)
                out_copy(c).start()

    pass_mate(0)
    send_queries(1)
    relay_own(0)
    send_own(2)
    relay_mate(0)
    pass_mate(1)
    relay_own(1)
    send_own(3)
    send_across(2)
    send_queries(2)

    def keep_ring_going(hp):
        if hp + 1 < HP:
            relay_mate(hp + 1)
        if hp + 2 < HP:
            pass_mate(hp + 2)
            relay_own(hp + 2)
        if hp == 0:
            send_across(3)
            send_queries(3)

    for hp in range(HP):
        complete(hp)
        visitors(hp)
        own_queries(hp)
        if hp :
            merge(hp - 1)
        if hp > 1:
            project_out(hp - 2)
    merge(HP - 1)
    project_out(HP - 2)

    project_out(HP - 1)

    tokens.wait_send()
    for hp in range(HP):
        hop(0, hp, own, at(other_row, x)).wait_send()
        hop(1, hp, own, at(z, right)).wait_send()
        hop(2, hp, own, at(z, left)).wait_send()
        hop(3, hp, mated, at(z, right)).wait_send()
        hop(4, hp, mated, at(z, left)).wait_send()
        hop(5, hp, own_left, at(z, right), 0).wait_send()
        hop(6, hp, own_right, at(z, left), 1).wait_send()
        hop(7, hp, mate_left, at(z, right), 0).wait_send()
        hop(8, hp, mate_right, at(z, left), 1).wait_send()
        att_copy(hp, core).wait_send()
    for k in range(SLOTS):
        @pl.when(pair > k)
        def _():
            for copy in meta_copies(k, q_slot[k]):
                copy.wait_send()
            for hp in range(HP):
                q_copy(k, hp, q_slot[k]).wait_send()

    @pl.loop(0, SLOTS)
    def _(slot):
        @pl.when(sender(slot) < ZS)
        def _():
            for hp in range(HP):
                for copy in partial_copies(hp, slot, pair):
                    copy.wait_send()

    for c in range(ow.shape[1] // 256):
        out_copy(c).wait()


def on_device(tokens, query_weight, key_weight, value_weight, out_weight, chosen):
    rows, half_d = tokens.shape
    width = query_weight.shape[1]
    out_half = out_weight.shape[1]
    row_table, device_table = tables()
    bf16, f32, i32 = jnp.bfloat16, jnp.float32, jnp.int32
    vmem = pltpu.VMEM
    dma = pltpu.SemaphoreType.DMA
    scratch = [vmem((SRC, 2, QB, BLOCK, PAIR), bf16) for _ in range(HP)] + [
        vmem((2, rows, half_d), bf16),
        vmem(query_weight.shape, bf16),
        vmem(key_weight.shape, bf16),
        vmem(value_weight.shape, bf16),
        vmem(out_weight.shape, bf16),
        vmem(chosen.shape, i32),
        vmem(row_table.shape, f32),
        vmem(device_table.shape, f32),
        vmem((2, ROWS, PAIR), f32),
        vmem((3, width // 256, ROWS, 256), f32),
        vmem((QB, ROWS), f32),
        vmem((ROWS, ROWS), f32),
        vmem((4, CAP * QB, OUT_KEYS), bf16),
        vmem((QB, ROWS), i32),
        vmem((SLOTS, CAP * QB, OUT_KEYS), bf16),
        vmem((SLOTS, QB, ROWS), i32),
        vmem((HP, SLOTS + 1, ROWS, PAIR), bf16),
        vmem((HP, SLOTS, ROWS, PAIR), bf16),
        vmem((HP, SLOTS, 8, PAIR), f32),
        vmem((HP, SLOTS, ROWS, PAIR), bf16),
        vmem((HP, SLOTS, 8, PAIR), f32),
        vmem((HP, ROWS, PAIR), f32),
        vmem((HP, 8, PAIR), f32),
        vmem((2, HP, ROWS, PAIR), bf16),
        vmem((rows, out_half), bf16),
        vmem((out_half // 256, rows, 256), f32),
        pltpu.SMEM((SLOTS + 1, QB, ROWS), i32),
        dma((8,)),
        dma((10, HP)),
        dma((10, HP)),
        dma((2,)),
        dma((SLOTS, HP)),
        dma((SLOTS, HP)),
        dma((SLOTS, 2)),
        dma((SLOTS, 2)),
        dma((SLOTS, HP)),
        dma((SLOTS, HP)),
        dma((SLOTS, HP)),
        dma((SLOTS, HP)),
        dma((SLOTS + 1,)),
        dma((out_half // 256,)),
    ]
    return pl.pallas_call(
        kernel,
        out_shape=jax.ShapeDtypeStruct((rows, out_half), bf16),
        in_specs=[pl.BlockSpec(memory_space=pl.ANY)] * 8,
        out_specs=pl.BlockSpec(memory_space=pl.ANY),
        scratch_shapes=scratch,
        compiler_params=pltpu.CompilerParams(
            collective_id=0, has_side_effects=True, vmem_limit_bytes=58 * 1024 * 1024
        ),
        name="block_attention",
    )(
        tokens, query_weight, key_weight, value_weight, out_weight, chosen,
        jnp.asarray(row_table), jnp.asarray(device_table),
    )


def solution(mesh):
    placed = (
        P(DP_KV, "tp"),
        P(None, "tp"),
        P(None, "tp"),
        P(None, "tp"),
        P(None, "tp"),
        P(DP_KV, None),
    )
    return jax.shard_map(
        on_device, mesh=mesh, in_specs=placed, out_specs=P(DP_KV, "tp"), check_vma=False
    )
```
